256 devices in a mesh: sp: 32 (over z, x), tp: 4 (over y), dp: 2 (over core).
Axes of the slice: x: 4, y: 4, z: 8, core: 2. Of those that a mesh axis runs over, the one named last changes fastest.
Arguments:
- latent_in: bfloat16 [24576, 2048], P(('dp', 'sp', 'tp')), parts along dimension 0, may hold values from -6 to 6
- condition: bfloat16 [4096], P(('dp', 'sp')), parts along dimension 0, may hold values from -8 to 8
- context_latent: bfloat16 [1024, 256], P(('dp', 'sp')), parts along dimension 0, may hold values from -6 to 6
- context_rope: bfloat16 [1024, 64], P(('dp', 'sp')), parts along dimension 0, may hold values from -6 to 6
- shift_weight: bfloat16 [2048, 2048], P('sp', 'tp'), may hold values from -0.125 to 0.125
- scale_weight: bfloat16 [2048, 2048], P('sp', 'tp'), may hold values from -0.125 to 0.125
- gate_weight: bfloat16 [2048, 2048], P('sp', 'tp'), may hold values from -0.125 to 0.125
- norm_gain: float32 [2048], replicated, may hold values from 0.1 to 1.9
- down_query: bfloat16 [2048, 512], replicated, may hold values from -0.125 to 0.125
- down_latent: bfloat16 [2048, 256], replicated, may hold values from -0.125 to 0.125
- down_rope: bfloat16 [2048, 64], replicated, may hold values from -0.125 to 0.125
- query_gain: float32 [512], replicated, may hold values from 0.5 to 60
- latent_gain: float32 [256], replicated, may hold values from 0.1 to 1.9
- up_query: bfloat16 [512, 1536], P(None, 'tp'), may hold values from -0.25 to 0.25
- up_key: bfloat16 [256, 1024], P(None, 'tp'), may hold values from -0.375 to 0.375
- up_value: bfloat16 [256, 1024], P(None, 'tp'), may hold values from -0.375 to 0.375
- context_bias: float32 [8], P('tp'), may hold values from 1 to 2.5
- out_weight: bfloat16 [1024, 2048], replicated, may hold values from -3 to 3
Outputs:
- mixed_out: bfloat16 [24576, 2048], P(('dp', 'sp', 'tp')), parts along dimension 0
The draws below stay inside these ranges and needn't reach their ends.
There are 2 independent parts, one for each index of `dp`. The reference program is written for one: setup_inputs(seed, part) draws one part's arguments, and reference() takes and returns one part's arrays. A program takes and returns all parts, laid end to end along the dimension named above; an argument that names none is the same for every part. Nothing has to cross between parts.
All inputs are finite; a program needn't handle non-finite values.
Results may differ from the reference program's by a relative error of at most 0.039.
The reference program's roundings to bfloat16 on the way count: a program that leaves them out, or rounds other values in their place, can miss the bound.
Values may be sent and summed in bfloat16 or wider, within the bound.
A program may use at most 128 MiB of HBM per device.

```python
import math
import jax
import jax.numpy as jnp
from jax import lax

D = 2048
HEADS = 8
QK_NOPE = 128
QK_ROPE = 64
V_HEAD = 128
Q_RANK = 512
KV_RANK = 256
GRID_W = 64
CTX = 512
TOKENS = 12288


def draw_query_gain(key, part):
    gains = jax.random.uniform(key, (Q_RANK,), jnp.float32, 0.5, 1.5)
    return gains


def levels(rng, shape, cuts, low, high):
    def one(axis_at, blocks):
        draws = jax.random.uniform(jax.random.fold_in(jax.random.fold_in(rng, 6), axis_at), (blocks,), jnp.float32, low / len(cuts), high / len(cuts))
        return jnp.repeat(jnp.exp(draws), shape[axis_at] // blocks).reshape((-1,) + (1,) * (len(shape) - axis_at - 1))

    gain = one(*cuts[0])
    for cut in cuts[1:]:
        gain = gain * one(*cut)
    return gain


def noise(own_key, extent, scale, reach, cuts=(), kind=jnp.bfloat16):
    level = levels(own_key, extent, cuts, -0.22, 0.18) if cuts else 1.0
    entries = jax.random.normal(own_key, extent, jnp.float32) * scale * level
    return jnp.minimum(jnp.maximum(entries, -reach), reach).astype(kind)


def setup_inputs(seed: int = 0, part: int = 0) -> dict:
    splits = jax.random.split(jax.random.key(seed), 19)
    part_splits = jax.random.split(jax.random.fold_in(splits[18], part), 19)
    latent_in = noise(part_splits[0], (TOKENS, D), 1.0, 6.0, ((0, 128),))
    condition = noise(part_splits[1], (D,), 2.0, 8.0, ((0, 32),))
    context_latent = noise(part_splits[2], (CTX, KV_RANK), 1.0, 6.0, ((0, 32),))
    context_rope = noise(part_splits[3], (CTX, QK_ROPE), 1.0, 6.0, ((0, 32),))
    shift_weight = noise(splits[4], (D, D), D ** -0.5, 0.125, ((0, 32), (1, 4)))
    scale_weight = noise(splits[5], (D, D), D ** -0.5, 0.125, ((0, 32), (1, 4)))
    gate_weight = noise(splits[6], (D, D), D ** -0.5, 0.125, ((0, 32), (1, 4)))
    norm_gain = jnp.clip(1.0 + 0.18 * jax.random.normal(splits[7], (D,), jnp.float32), 0.1, 1.9)
    down_query = noise(splits[8], (D, Q_RANK), D ** -0.5, 0.125)
    down_latent = noise(splits[9], (D, KV_RANK), D ** -0.5, 0.125)
    down_rope = noise(splits[10], (D, QK_ROPE), D ** -0.5, 0.125)
    query_gain = draw_query_gain(jax.random.fold_in(splits[18], 71), part)
    latent_gain = jnp.clip(1.0 + 0.18 * jax.random.normal(splits[12], (KV_RANK,), jnp.float32), 0.1, 1.9)
    up_query = noise(splits[13], (Q_RANK, HEADS * (QK_NOPE + QK_ROPE)), Q_RANK ** -0.5, 0.25, ((1, 4),))
    up_key = noise(splits[14], (KV_RANK, HEADS * QK_NOPE), KV_RANK ** -0.5, 0.375, ((1, 4),))
    up_value = noise(splits[15], (KV_RANK, HEADS * V_HEAD), KV_RANK ** -0.5, 0.375, ((1, 4),))
    context_bias = jnp.clip(1.0 + 1.5 * jax.random.uniform(splits[16], (HEADS,), jnp.float32) ** levels(splits[16], (HEADS,), ((0, 4),), -0.2, 0.2), 1.0, 2.5)
    out_weight = noise(splits[17], (HEADS * V_HEAD, D), 0.5, 3.0)
    return dict(latent_in=latent_in, condition=condition, context_latent=context_latent, context_rope=context_rope, shift_weight=shift_weight, scale_weight=scale_weight, gate_weight=gate_weight, norm_gain=norm_gain, down_query=down_query, down_latent=down_latent, down_rope=down_rope, query_gain=query_gain, latent_gain=latent_gain, up_query=up_query, up_key=up_key, up_value=up_value, context_bias=context_bias, out_weight=out_weight)


epsilon = 1e-06
rope_base = 10000.0

def rms_scaled(values, gain_vec):
    mean_sq = lax.optimization_barrier(jnp.mean(values * values, axis=-1, keepdims=True))
    return values * lax.rsqrt(mean_sq + epsilon) * gain_vec

def rope_tables(positions, rope_width):
    freq_count = rope_width // 4
    inverse = rope_base ** (-jnp.arange(freq_count, dtype=jnp.float32) / freq_count)
    grid_row = (positions // GRID_W).astype(jnp.float32)
    grid_col = (positions % GRID_W).astype(jnp.float32)
    row_angle = grid_row[:, None] * inverse
    col_angle = grid_col[:, None] * inverse
    angles = jnp.concatenate([row_angle, row_angle, col_angle, col_angle], axis=-1)
    return (jnp.cos(angles), jnp.sin(angles))

def rope_turn(values, cosine_table, sine_table):
    part_one, part_two, part_three, part_four = jnp.split(values, 4, axis=-1)
    turned = jnp.concatenate([-part_two, part_one, -part_four, part_three], axis=-1)
    return values * cosine_table + turned * sine_table

def reference(latent_in, condition, context_latent, context_rope, shift_weight, scale_weight, gate_weight, norm_gain, down_query, down_latent, down_rope, query_gain, latent_gain, up_query, up_key, up_value, context_bias, out_weight):
    activated = jax.nn.silu(condition.astype(jnp.float32)).astype(jnp.bfloat16)
    shift_vec = jnp.dot(activated, shift_weight, preferred_element_type=jnp.float32)
    scale_vec = jnp.dot(activated, scale_weight, preferred_element_type=jnp.float32)
    gate_vec = jnp.dot(activated, gate_weight, preferred_element_type=jnp.float32)
    residual_in = latent_in.astype(jnp.float32)
    normed = (rms_scaled(residual_in, norm_gain) * (1.0 + scale_vec) + shift_vec).astype(jnp.bfloat16)
    query_low = rms_scaled(jnp.dot(normed, down_query, preferred_element_type=jnp.float32), query_gain).astype(jnp.bfloat16)
    latent_low = rms_scaled(jnp.dot(normed, down_latent, preferred_element_type=jnp.float32), latent_gain).astype(jnp.bfloat16)
    positions = jnp.arange(TOKENS, dtype=jnp.int32)
    cosine_table, sine_table = rope_tables(positions, QK_ROPE)
    rope_keys = rope_turn(jnp.dot(normed, down_rope, preferred_element_type=jnp.float32), cosine_table, sine_table).astype(jnp.bfloat16)
    queries = jnp.dot(query_low, up_query, preferred_element_type=jnp.float32).reshape(TOKENS, HEADS, QK_NOPE + QK_ROPE)
    query_rope = rope_turn(queries[:, :, QK_NOPE:], cosine_table[:, None, :], sine_table[:, None, :])
    queries = jnp.concatenate([queries[:, :, :QK_NOPE], query_rope], axis=-1).astype(jnp.bfloat16)
    all_latent = jnp.concatenate([context_latent, latent_low], axis=0)
    all_rope = jnp.concatenate([context_rope, rope_keys], axis=0)
    key_count = CTX + TOKENS
    keys_nope = jnp.dot(all_latent, up_key, preferred_element_type=jnp.float32).astype(jnp.bfloat16).reshape(key_count, HEADS, QK_NOPE)
    values_all = jnp.dot(all_latent, up_value, preferred_element_type=jnp.float32).astype(jnp.bfloat16).reshape(key_count, HEADS, V_HEAD)
    bias_row = jnp.concatenate([jnp.broadcast_to(context_bias[:, None], (HEADS, CTX)), jnp.zeros((HEADS, TOKENS), jnp.float32)], axis=1)[:, None, :]
    keys_wide = keys_nope.astype(jnp.float32)
    rope_wide = all_rope.astype(jnp.float32)
    values_wide = values_all.astype(jnp.float32)
    block_rows = math.gcd(TOKENS, 512)
    query_blocks = queries.astype(jnp.float32).reshape(TOKENS // block_rows, block_rows, HEADS, QK_NOPE + QK_ROPE)
    score_scale = (QK_NOPE + QK_ROPE) ** (-0.5)

    def one_block(query_block):
        scores = jnp.einsum('thd,khd->htk', query_block[:, :, :QK_NOPE], keys_wide)
        scores = scores + jnp.einsum('thr,kr->htk', query_block[:, :, QK_NOPE:], rope_wide)
        scores = scores * score_scale + bias_row
        row_max = lax.optimization_barrier(jnp.max(scores, axis=-1, keepdims=True))
        weights = jnp.exp(scores - row_max)
        totals = lax.optimization_barrier(jnp.sum(weights, axis=-1))
        rounded = lax.optimization_barrier(weights.astype(jnp.bfloat16)).astype(jnp.float32)
        summed = jnp.einsum('htk,khd->htd', rounded, values_wide)
        return (summed / totals[:, :, None]).astype(jnp.bfloat16)
    outputs = lax.map(one_block, query_blocks)
    attended = outputs.transpose(0, 2, 1, 3).reshape(TOKENS, HEADS * V_HEAD)
    mixed = jnp.dot(attended, out_weight, preferred_element_type=jnp.float32)
    return (residual_in + gate_vec * mixed).astype(jnp.bfloat16)
```

```python
import functools
import math

import jax
import jax.numpy as jnp
from jax import lax
from jax.experimental import pallas as pl
from jax.experimental.pallas import tpu as pltpu
from jax.sharding import Mesh
from jax.sharding import PartitionSpec as P

ROWS = 96
D = 2048
NZ, NX, NY = 8, 4, 4
GRID_W = 64
CTXK = 128
EPS = 1e-06
QN = NY * ROWS
BUNDLE = NX * ROWS
LOG2E = math.log2(math.e)
SCALE2 = LOG2E / math.sqrt(192.0)
MESH = pl.DeviceIdType.MESH
F32 = jnp.float32
BF16 = jnp.bfloat16
NEG = float("-inf")


def dot(a, b):
    return jnp.dot(a, b, preferred_element_type=F32)


def dot_nt(a, b):
    return lax.dot_general(a, b, (((1,), (1,)), ((), ())), preferred_element_type=F32)


def remote(src, dst, send_sem, recv_sem, **where):
    return pltpu.make_async_remote_copy(
        src_ref=src, dst_ref=dst, send_sem=send_sem, recv_sem=recv_sem,
        device_id=where, device_id_type=MESH,
    )


def greet(peers):
    barrier = pltpu.get_barrier_semaphore()
    for where in peers:
        pl.semaphore_signal(barrier, inc=1, device_id=where, device_id_type=MESH)
    pl.semaphore_wait(barrier, len(peers))


def prepare_kernel(
    cond, sw, cw, gw, bias, lat, gain, qg, lg, cosr, sinr, ctxl, ctxr,
    dq_h, dl_h, dr_h, uq_h, uk_h, uv_h,
    qlow_o, kblk_o, gate_o, bias_o, ctx_o, uq, uk, uv,
    dq, dl, dr, mod_x, mod_z, mod_y, cblk, cx,
    down_sem, own_sem, xs, xr, zs, zr, ys, yr, cxs, cxr, czs, czr, ws, wr, fs, fr,
):
    z, x, y, c = (lax.axis_index(n) for n in ("z", "x", "y", "c"))
    downs = [
        pltpu.make_async_copy(h, v, down_sem.at[i])
        for i, (h, v) in enumerate(((dq_h, dq), (dl_h, dl), (dr_h, dr)))
    ]
    owns = [
        pltpu.make_async_copy(h, v.at[y], own_sem.at[i])
        for i, (h, v) in enumerate(((uq_h, uq), (uk_h, uk), (uv_h, uv)))
    ]
    for copy in owns + downs:
        copy.start()
    xp = [lax.rem(x + d, NX) for d in range(NX)]
    yp = [lax.rem(y + d, NY) for d in range(NY)]
    zp = [lax.rem(z + d, NZ) for d in range(NZ)]
    greet(
        [{"x": xp[d]} for d in range(1, NX)]
        + [{"y": yp[d]} for d in range(1, NY)]
        + [{"z": zp[d]} for d in range(1, NZ)]
        + [{"c": 1 - c}]
    )
    v = cond[...].astype(F32)
    activated = (v / (1.0 + jnp.exp(-v))).astype(BF16)
    part = jnp.concatenate([dot(activated, w[...]) for w in (sw, cw, gw)], axis=0)
    mod_x[x] = part
    xcopies = [
        remote(mod_x.at[x], mod_x.at[x], xs.at[d], xr.at[d], x=xp[d]) for d in range(1, NX)
    ]
    for copy in xcopies:
        copy.start()
    cblk[...] = jnp.concatenate(
        [ctxl[...], ctxr[...], jnp.zeros((16, 64), BF16)], axis=1
    )
    cx[x] = cblk[...]
    ccopies = [remote(cblk, cx.at[x], cxs.at[d], cxr.at[d], x=xp[d]) for d in range(1, NX)]
    for copy in ccopies:
        copy.start()
    for copy in owns:
        copy.wait()

    def half(ref, slot, core):
        rows = ref.shape[1] // 2
        return ref.at[slot, pl.ds(pl.multiple_of(core * rows, rows), rows)]

    wcopies = [
        [
            remote(half(w, y, c), half(w, y, c), ws.at[d, i], wr.at[d, i], y=yp[d])
            for i, w in enumerate((uq, uk, uv))
        ]
        for d in range(1, NY)
    ]
    for copy in xcopies:
        copy.wait_recv()
    mod_z[z] = mod_x[0] + mod_x[1] + mod_x[2] + mod_x[3]
    zcopies = [
        remote(mod_z.at[z], mod_z.at[z], zs.at[d], zr.at[d], z=zp[d]) for d in range(1, NZ)
    ]
    for copy in zcopies:
        copy.start()
    for d in (1, 3):
        wcopies[d - 1][0].start()
    lat32 = lat[...].astype(F32)
    inv = lax.rsqrt(jnp.mean(lat32 * lat32, axis=-1, keepdims=True) + EPS)
    for copy in ccopies:
        copy.wait_recv()
    mine = z // 2 == y
    first = (z % 2) * 64
    zc = [
        remote(
            cx, ctx_o.at[pl.ds(pl.multiple_of((z % 2) * NX, NX), NX)], czs.at[d],
            czr.at[z % 2], z=zp[d],
        )
        for d in range(1, NZ)
    ]

    @pl.when(mine)
    def _():
        ctx_o[pl.ds((z % 2) * NX, NX)] = cx[...]
        for copy in zc:
            copy.start()

    for copy in zcopies:
        copy.wait_recv()
    total = mod_z[0]
    for k in range(1, NZ):
        total = total + mod_z[k]
    lane = lax.broadcasted_iota(jnp.int32, (1, 512), 1)
    bias_row = jnp.where(lane == 0, bias[0], jnp.where(lane == 1, bias[1], 0.0))
    mod_y[y] = jnp.concatenate([total, bias_row], axis=0)
    ycopies = [
        remote(mod_y.at[y], mod_y.at[y], ys.at[d], yr.at[d], y=yp[d]) for d in range(1, NY)
    ]
    for copy in ycopies:
        copy.start()
    for d in (1, 3):
        for i in (1, 2):
            wcopies[d - 1][i].start()
    for copy in wcopies[1]:
        copy.start()
    for copy in ycopies:
        copy.wait_recv()
    shift = jnp.concatenate([mod_y[k, 0:1] for k in range(NY)], axis=1)
    scale = jnp.concatenate([mod_y[k, 1:2] for k in range(NY)], axis=1)
    gate_o[...] = jnp.concatenate([mod_y[k, 2:3] for k in range(NY)], axis=1)
    bias_o[...] = jnp.concatenate([mod_y[k, 3:4, 0:128] for k in range(NY)], axis=0)
    normed = (lat32 * inv * gain[...] * (1.0 + scale) + shift).astype(BF16)
    for copy in downs:
        copy.wait()

    def rms(a, g):
        return a * lax.rsqrt(jnp.mean(a * a, axis=-1, keepdims=True) + EPS) * g

    qlow_o[...] = rms(dot(normed, dq[...]), qg[...]).astype(BF16)
    low = rms(dot(normed, dl[...]), lg[...]).astype(BF16)
    u = dot(normed, dr[...])
    turned = jnp.concatenate([-u[:, 16:32], u[:, 0:16], -u[:, 48:64], u[:, 32:48]], axis=1)
    rope = (u * cosr[...] + turned * sinr[...]).astype(BF16)
    kblk_o[...] = jnp.concatenate([low, rope, jnp.zeros((ROWS, 64), BF16)], axis=1)
    forwards = []
    for d in (1, 3, 2):
        slot = lax.rem(y - d + NY, NY)
        for i, w in enumerate((uq, uk, uv)):
            wcopies[d - 1][i].wait_recv()
            copy = remote(half(w, slot, c), half(w, slot, c), fs.at[d, i], fr.at[d, i], c=1 - c)
            copy.start()
            forwards.append(copy)
    for copy in forwards:
        copy.wait()

    for k in range(2):
        @pl.when(z != 2 * y + k)
        def _():
            remote(cx, ctx_o.at[pl.ds(k * NX, NX)], czs.at[0], czr.at[k], z=zp[1]).wait_recv()

    @pl.when(mine)
    def _():
        for copy in zc:
            copy.wait_send()

    for copy in xcopies + ccopies + zcopies + ycopies + sum(wcopies, []):
        copy.wait_send()


def attend_kernel(
    qlow, kblk, uq, uk, uv, ctx, bias, cos_t, sin_t,
    out,
    qa, zk, wq_t, wv_t, q_t, m_s, l_s, acc, ob, rb, lse, sb, rsb,
    qs, qr, xs, xr, rs, rr, ls, lr, os, orr, ss, sr,
):
    z, x, y = (lax.axis_index(n) for n in ("z", "x", "y"))
    xp = [lax.rem(x + d, NX) for d in range(NX)]
    yp = [lax.rem(y + d, NY) for d in range(NY)]
    right, left = lax.rem(z + 1, NZ), lax.rem(z + NZ - 1, NZ)
    greet(
        [{"x": xp[d]} for d in range(1, NX)]
        + [{"y": yp[d]} for d in range(1, NY)]
        + [{"z": right}, {"z": left}]
    )
    kcopies = [
        remote(kblk, zk.at[z, x], xs.at[d], xr.at[d], x=xp[d]) for d in range(1, NX)
    ]
    qcopies = [remote(qlow, qa.at[y], qs.at[d], qr.at[d], y=yp[d]) for d in range(1, NY)]
    for copy in kcopies + qcopies:
        copy.start()
    qa[y] = qlow[...]
    zk[z, x] = kblk[...]
    for k in range(NY):
        wq_t[k] = uq[k].T
        wv_t[k] = uv[k].T
    m_s[...] = jnp.full(m_s.shape, NEG, F32)
    l_s[...] = jnp.zeros(l_s.shape, F32)
    acc[...] = jnp.zeros(acc.shape, F32)

    for copy in kcopies:
        copy.wait_recv()

    def slot_of(offset):
        return lax.rem(z + offset + NZ, NZ)

    def send_right(s):
        k = slot_of(1 - s)
        return remote(zk.at[k], zk.at[k], rs.at[s], rr.at[s], z=right)

    def send_left(s):
        k = slot_of(s - 1)
        return remote(zk.at[k], zk.at[k], ls.at[s], lr.at[s], z=left)

    last_right = remote(
        zk.at[slot_of(-3), pl.ds(0, 2)], zk.at[slot_of(-3), pl.ds(0, 2)],
        rs.at[4], rr.at[4], z=right,
    )
    last_left = remote(
        zk.at[slot_of(3), pl.ds(2, 2)], zk.at[slot_of(3), pl.ds(2, 2)],
        ls.at[4], lr.at[4], z=left,
    )
    send_right(1).start()
    send_left(1).start()

    for copy in qcopies:
        copy.wait_recv()

    @pl.loop(0, NY)
    def _(k):
        qt = dot_nt(wq_t[k], qa[...].reshape(QN, 512))
        for h in range(2):
            b = 192 * h
            u = qt[b + 128 : b + 192]
            turned = jnp.concatenate([-u[16:32], u[0:16], -u[48:64], u[32:48]], axis=0)
            rope = u * cos_t[...] + turned * sin_t[...]
            q_t[2 * k + h] = jnp.concatenate(
                [qt[b : b + 128], rope, jnp.zeros((64, QN), F32)], axis=0
            ).astype(BF16)

    def process(load, biased):
        @pl.loop(0, NY)
        def _(k):
            keys = load()
            low, rope = keys[:, :256], keys[:, 256:]
            nope = dot(low, uk[k]).astype(BF16)
            val_t = dot_nt(wv_t[k], low).astype(BF16)
            for h in range(2):
                head = 2 * k + h
                key = jnp.concatenate([nope[:, 128 * h : 128 * h + 128], rope], axis=1)
                s = dot(key, q_t[head]) * SCALE2
                if biased:
                    s = s + bias[pl.ds(k, 1), h : h + 1] * LOG2E
                m_old = m_s[head]
                m_new = jnp.maximum(m_old, jnp.max(s, axis=0, keepdims=True))
                p = jnp.exp2(s - m_new)
                shrink = jnp.exp2(m_old - m_new)
                l_s[head] = l_s[head] * shrink + jnp.sum(p, axis=0, keepdims=True)
                acc[head] = acc[head] * shrink + dot(
                    val_t[128 * h : 128 * h + 128], p.astype(BF16)
                )
                m_s[head] = m_new

    process(lambda: ctx[...].reshape(CTXK, 384), True)
    process(lambda: zk[z].reshape(BUNDLE, 384), False)

    @pl.loop(1, 4)
    def _(s):
        send_right(s).wait_recv()
        send_left(s).wait_recv()

        @pl.when(s < 3)
        def _():
            send_right(s + 1).start()
            send_left(s + 1).start()

        @pl.when(s == 3)
        def _():
            last_right.start()
            last_left.start()

        process(
            lambda: jnp.concatenate(
                [zk[slot_of(-s)].reshape(BUNDLE, 384), zk[slot_of(s)].reshape(BUNDLE, 384)],
                axis=0,
            ),
            False,
        )

    last_right.wait_recv()
    last_left.wait_recv()
    process(lambda: zk[slot_of(4)].reshape(BUNDLE, 384), False)

    for k in range(NY):
        both = []
        for h in range(2):
            head = 2 * k + h
            total = l_s[head]
            both.append((acc[head] / total).T)
            lse[head : head + 1] = m_s[head] + jnp.log2(total)
        ob[k] = jnp.concatenate(both, axis=1).astype(BF16).reshape(NY, ROWS, 256)
        for d in range(1, NY):
            remote(ob.at[k, yp[d]], rb.at[d, k], os.at[d, k], orr.at[d, k], y=yp[d]).start()
    sb[...] = jnp.concatenate([lse[...], jnp.zeros((120, QN), F32)], axis=0).T.reshape(
        NY, ROWS, 128
    )
    for d in range(1, NY):
        remote(sb.at[yp[d]], rsb.at[d], ss.at[d], sr.at[d], y=yp[d]).start()
    for d in range(1, NY):
        remote(sb.at[yp[d]], rsb.at[d], ss.at[d], sr.at[d], y=yp[d]).wait_recv()
    stats = [sb[y]] + [rsb[d] for d in range(1, NY)]
    top = jnp.maximum(jnp.maximum(stats[0], stats[1]), jnp.maximum(stats[2], stats[3]))
    raised = [jnp.exp2(s - top) for s in stats]
    whole = raised[0] + raised[1] + raised[2] + raised[3]
    shares = [r / whole for r in raised]
    for k in range(NY):
        for d in range(1, NY):
            remote(ob.at[k, yp[d]], rb.at[d, k], os.at[d, k], orr.at[d, k], y=yp[d]).wait_recv()
        pieces = [ob[k, y]] + [rb[d, k] for d in range(1, NY)]
        for h in range(2):
            head = 2 * k + h
            value = sum(
                piece[:, 128 * h : 128 * h + 128].astype(F32) * share[:, head : head + 1]
                for piece, share in zip(pieces, shares)
            )
            out[:, 128 * head : 128 * head + 128] = value.astype(BF16)

    for copy in kcopies + qcopies + [last_right, last_left]:
        copy.wait_send()

    @pl.loop(1, 4)
    def _(s):
        send_right(s).wait_send()
        send_left(s).wait_send()

    for d in range(1, NY):
        remote(sb.at[yp[d]], rsb.at[d], ss.at[d], sr.at[d], y=yp[d]).wait_send()
        for k in range(NY):
            remote(ob.at[k, yp[d]], rb.at[d, k], os.at[d, k], orr.at[d, k], y=yp[d]).wait_send()


def tables(tokens):
    inverse = 10000.0 ** (-jnp.arange(16, dtype=F32) / 16)
    row = (tokens // GRID_W).astype(F32)
    col = (tokens % GRID_W).astype(F32)
    return row, col, inverse


def on_device(
    latent_in, condition, context_latent, context_rope, shift_weight, scale_weight, gate_weight,
    norm_gain, down_query, down_latent, down_rope, query_gain, latent_gain, up_query, up_key,
    up_value, context_bias, out_weight,
):
    sp = lax.axis_index("z") * NX + lax.axis_index("x")
    own = (sp * NY + lax.axis_index("y")) * ROWS + jnp.arange(ROWS, dtype=jnp.int32)
    row, col, inverse = tables(own)
    ra, ca = row[:, None] * inverse, col[:, None] * inverse
    own_angles = jnp.concatenate([ra, ra, ca, ca], axis=1)
    row, col, inverse = tables(sp * QN + jnp.arange(QN, dtype=jnp.int32))
    ra, ca = inverse[:, None] * row, inverse[:, None] * col
    line_angles = jnp.concatenate([ra, ra, ca, ca], axis=0)

    vmem = pl.BlockSpec(memory_space=pltpu.VMEM)
    smem = pl.BlockSpec(memory_space=pltpu.SMEM)
    hbm = pl.BlockSpec(memory_space=pl.ANY)
    dma = pltpu.SemaphoreType.DMA
    shape = jax.ShapeDtypeStruct
    qlow, kblk, gate, bias, ctx, uq, uk, uv = pl.pallas_call(
        prepare_kernel,
        name="prepare",
        out_shape=(
            shape((ROWS, 512), BF16),
            shape((ROWS, 384), BF16),
            shape((1, D), F32),
            shape((NY, 128), F32),
            shape((8, 16, 384), BF16),
            shape((NY, 512, 384), BF16),
            shape((NY, 256, 256), BF16),
            shape((NY, 256, 256), BF16),
        ),
        in_specs=[vmem] * 4 + [smem] + [vmem] * 8 + [hbm] * 6,
        out_specs=(vmem,) * 8,
        scratch_shapes=[
            pltpu.VMEM((D, 512), BF16),
            pltpu.VMEM((D, 256), BF16),
            pltpu.VMEM((D, 64), BF16),
            pltpu.VMEM((NX, 3, 512), F32),
            pltpu.VMEM((NZ, 3, 512), F32),
            pltpu.VMEM((NY, 4, 512), F32),
            pltpu.VMEM((16, 384), BF16),
            pltpu.VMEM((NX, 16, 384), BF16),
            dma((3,)), dma((3,)),
            dma((NX,)), dma((NX,)),
            dma((NZ,)), dma((NZ,)),
            dma((NY,)), dma((NY,)),
            dma((NX,)), dma((NX,)),
            dma((NZ,)), dma((2,)),
            dma((NY, 3)), dma((NY, 3)),
            dma((NY, 3)), dma((NY, 3)),
        ],
        compiler_params=pltpu.CompilerParams(
            collective_id=0, has_side_effects=True, vmem_limit_bytes=48 * 1024 * 1024
        ),
    )(
        condition.reshape(1, -1), shift_weight, scale_weight, gate_weight, context_bias,
        latent_in, norm_gain.reshape(1, -1), query_gain.reshape(1, -1),
        latent_gain.reshape(1, -1), jnp.cos(own_angles), jnp.sin(own_angles),
        context_latent, context_rope, down_query, down_latent, down_rope,
        up_query, up_key, up_value,
    )
    attended = pl.pallas_call(
        attend_kernel,
        name="attend",
        out_shape=shape((ROWS, 1024), BF16),
        in_specs=[vmem] * 9,
        out_specs=vmem,
        scratch_shapes=[
            pltpu.VMEM((NY, ROWS, 512), BF16),
            pltpu.VMEM((NZ, NX, ROWS, 384), BF16),
            pltpu.VMEM((NY, 384, 512), BF16),
            pltpu.VMEM((NY, 256, 256), BF16),
            pltpu.VMEM((8, 256, QN), BF16),
            pltpu.VMEM((8, 1, QN), F32),
            pltpu.VMEM((8, 1, QN), F32),
            pltpu.VMEM((8, 128, QN), F32),
            pltpu.VMEM((NY, NY, ROWS, 256), BF16),
            pltpu.VMEM((NY, NY, ROWS, 256), BF16),
            pltpu.VMEM((8, QN), F32),
            pltpu.VMEM((NY, ROWS, 128), F32),
            pltpu.VMEM((NY, ROWS, 128), F32),
            dma((NY,)), dma((NY,)),
            dma((NX,)), dma((NX,)),
            dma((5,)), dma((5,)),
            dma((5,)), dma((5,)),
            dma((NY, NY)), dma((NY, NY)),
            dma((NY,)), dma((NY,)),
        ],
        compiler_params=pltpu.CompilerParams(
            collective_id=1, has_side_effects=True, vmem_limit_bytes=56 * 1024 * 1024
        ),
    )(qlow, kblk, uq, uk, uv, ctx, bias, jnp.cos(line_angles), jnp.sin(line_angles))
    mixed = jnp.dot(attended, out_weight, preferred_element_type=F32)
    return (latent_in.astype(F32) + gate * mixed).astype(BF16)


def solution(mesh):
    split = Mesh(mesh.devices.reshape(NZ, NX, NY, 2), ("z", "x", "y", "c"))
    rows = P(("c", "z", "x", "y"), None)
    held = P(("c", "z", "x"), None)
    weight = P(("z", "x"), "y")
    placed = (
        rows, P(("c", "z", "x")), held, held, weight, weight, weight, P(), P(), P(), P(), P(),
        P(), P(None, "y"), P(None, "y"), P(None, "y"), P("y"), P(),
    )
    return jax.shard_map(
        on_device, mesh=split, in_specs=placed, out_specs=rows, check_vma=False
    )
```

```python
import math

import jax
import jax.numpy as jnp
import numpy as np
from jax import lax
from jax.experimental import pallas as pl
from jax.experimental.pallas import tpu as pltpu
from jax.sharding import Mesh
from jax.sharding import PartitionSpec as P

ROWS = 96
D = 2048
NZ, NX, NY = 8, 4, 4
GRID_W = 64
CTXK = 128
EPS = 1e-06
QN = NY * ROWS
BUNDLE = NX * ROWS
LOG2E = math.log2(math.e)
SCALE2 = LOG2E / math.sqrt(192.0)
MESH = pl.DeviceIdType.MESH
F32 = jnp.float32
BF16 = jnp.bfloat16
NEG = float("-inf")


def dot(a, b):
    return jnp.dot(a, b, preferred_element_type=F32)


def dot_nt(a, b):
    return lax.dot_general(a, b, (((1,), (1,)), ((), ())), preferred_element_type=F32)


def remote(src, dst, send_sem, recv_sem, **where):
    return pltpu.make_async_remote_copy(
        src_ref=src, dst_ref=dst, send_sem=send_sem, recv_sem=recv_sem,
        device_id=where, device_id_type=MESH,
    )


def greet(peers):
    barrier = pltpu.get_barrier_semaphore()
    for where in peers:
        pl.semaphore_signal(barrier, inc=1, device_id=where, device_id_type=MESH)
    pl.semaphore_wait(barrier, len(peers))


def piece_order(k):
    return k + (k // 2) * (5 - 2 * k)


def kernel(
    cond_h, sw_h, cw_h, gw_h, bias_h, lat_h, gain_h, qg_h, lg_h, rowt_h, colt_h, ctxl_h, ctxr_h,
    dq_h, dl_h, dr_h, uq_h, uk_h, uv_h, ow_h,
    out,
    cond, sw, cw, gw, bias, lat, gain, qg, lg, rowt, colt, ctxl, ctxr, dq, dl, dr, ow,
    uq, uk, uv, mod_x, mod_z, mod_y, cblk, cx, ctx, kblk, qlow, gate_s, bias_s,
    qa, zk, wq_t, wv_t, q_t, kn, vt, sa, sb, m_s, l_s, acc, ob, rb, st, rst, mixed,
    in_sem, own_sem, xs, xr, zs, zr, ys, yr, cxs, cxr, czs, czr, ws, wr, hs, hr, fs, fr,
    ks, kr, qs, qr, rs, rr, ls, lr, os, orr, ss, sr,
):
    z, x, y, c = (lax.axis_index(n) for n in ("z", "x", "y", "c"))
    sp = z * NX + x
    fetches = [
        pltpu.make_async_copy(h, v, in_sem.at[i])
        for i, (h, v) in enumerate((
            (cond_h, cond), (sw_h, sw), (cw_h, cw), (gw_h, gw), (bias_h, bias), (ctxl_h, ctxl),
            (ctxr_h, ctxr), (lat_h, lat), (gain_h, gain), (qg_h, qg), (lg_h, lg),
            (rowt_h, rowt), (colt_h, colt), (dq_h, dq), (dl_h, dl), (dr_h, dr), (ow_h, ow),
        ))
    ]
    owns = [
        pltpu.make_async_copy(h, v.at[y], own_sem.at[i])
        for i, (h, v) in enumerate(((uq_h, uq), (uk_h, uk), (uv_h, uv)))
    ]
    for copy in fetches[:8] + owns + fetches[8:]:
        copy.start()
    xp = [lax.rem(x + d, NX) for d in range(NX)]
    yp = [lax.rem(y + d, NY) for d in range(NY)]
    zp = [lax.rem(z + d, NZ) for d in range(NZ)]
    right, left = zp[1], zp[NZ - 1]
    greet(
        [{"x": xp[d]} for d in range(1, NX)]
        + [{"y": yp[d]} for d in range(1, NY)]
        + [{"z": zp[d]} for d in range(1, NZ)]
        + [{"c": 1 - c}]
    )

    for copy in fetches[:7]:
        copy.wait()
    v = cond[...].astype(F32)
    activated = (v / (1.0 + jnp.exp(-v))).astype(BF16)
    mod_x[x] = jnp.concatenate([dot(activated, w[...]) for w in (sw, cw, gw)], axis=0)
    xcopies = [
        remote(mod_x.at[x], mod_x.at[x], xs.at[d], xr.at[d], x=xp[d]) for d in range(1, NX)
    ]
    for copy in xcopies:
        copy.start()
    cblk[...] = jnp.concatenate([ctxl[...], ctxr[...], jnp.zeros((16, 64), BF16)], axis=1)
    cx[x] = cblk[...]
    ccopies = [remote(cblk, cx.at[x], cxs.at[d], cxr.at[d], x=xp[d]) for d in range(1, NX)]
    for copy in ccopies:
        copy.start()

    for copy in owns:
        copy.wait()

    def half(ref, slot):
        rows = ref.shape[1] // 2
        return ref.at[slot, pl.ds(pl.multiple_of(c * rows, rows), rows)]

    ups = (uq, uk, uv)
    after = [
        remote(half(w, y), half(w, y), ws.at[0, i], wr.at[0, i], y=yp[1])
        for i, w in enumerate(ups)
    ]
    before = [
        remote(half(w, y), half(w, y), ws.at[1, i], wr.at[1, i], y=yp[3])
        for i, w in enumerate(ups)
    ]
    hops = [
        remote(half(uq, yp[3]), half(uq, yp[3]), hs.at[0], hr.at[0], y=yp[1]),
        remote(half(uk, yp[1]), half(uk, yp[1]), hs.at[1], hr.at[1], y=yp[3]),
        remote(half(uv, yp[1]), half(uv, yp[1]), hs.at[2], hr.at[2], y=yp[3]),
    ]

    def across(slot, d, i):
        return remote(half(ups[i], slot), half(ups[i], slot), fs.at[d, i], fr.at[d, i], c=1 - c)

    after[0].start()
    before[0].start()
    after[1].start()
    before[1].start()

    for copy in xcopies:
        copy.wait_recv()
    mod_z[z] = mod_x[0] + mod_x[1] + mod_x[2] + mod_x[3]
    zcopies = [
        remote(mod_z.at[z], mod_z.at[z], zs.at[d], zr.at[d], z=zp[d]) for d in range(1, NZ)
    ]
    for copy in zcopies:
        copy.start()
    for copy in fetches[7:13]:
        copy.wait()
    lat32 = lat[...].astype(F32)
    inv = lax.rsqrt(jnp.mean(lat32 * lat32, axis=-1, keepdims=True) + EPS)
    scaled = lat32 * inv * gain[...]
    line = [rowt[pl.ds(sp * 6 + i, 1), :] + colt[...] for i in range(6)]
    line_t = jnp.concatenate(line, axis=0).T
    own_table = []
    for t in range(3):
        g = y * 3 + t
        own_table.append(
            rowt[pl.ds(sp * 6 + g // 2, 1), :]
            + colt[pl.ds(pl.multiple_of((g % 2) * 32, 32), 32), :]
        )
    own_table = jnp.concatenate(own_table, axis=0)
    wq_t[y] = uq[y].T
    wv_t[y] = uv[y].T
    m_s[...] = jnp.full(m_s.shape, NEG, F32)
    l_s[...] = jnp.zeros(l_s.shape, F32)
    acc[...] = jnp.zeros(acc.shape, F32)
    for copy in ccopies:
        copy.wait_recv()
    mine = z // 2 == y
    zc = [
        remote(
            cx, ctx.at[pl.ds(pl.multiple_of((z % 2) * NX, NX), NX)], czs.at[d],
            czr.at[z % 2], z=zp[d],
        )
        for d in range(1, NZ)
    ]

    @pl.when(mine)
    def _():
        ctx[pl.ds((z % 2) * NX, NX)] = cx[...]
        for copy in zc:
            copy.start()

    for copy in zcopies:
        copy.wait_recv()
    total = mod_z[0]
    for k in range(1, NZ):
        total = total + mod_z[k]
    bias_row = jnp.concatenate([bias[...], jnp.zeros((1, 510), F32)], axis=1)
    mod_y[y] = jnp.concatenate([total, bias_row], axis=0)
    ycopies = [
        remote(mod_y.at[y], mod_y.at[y], ys.at[d], yr.at[d], y=yp[d]) for d in range(1, NY)
    ]
    for copy in ycopies:
        copy.start()
    after[0].wait_recv()
    hops[0].start()
    across(yp[3], 0, 0).start()
    before[0].wait_recv()
    across(yp[1], 1, 0).start()
    before[1].wait_recv()
    hops[1].start()
    across(yp[1], 1, 1).start()
    after[1].wait_recv()
    across(yp[3], 0, 1).start()
    before[2].start()
    after[2].start()

    for copy in ycopies:
        copy.wait_recv()
    shift = jnp.concatenate([mod_y[k, 0:1] for k in range(NY)], axis=1)
    scale = jnp.concatenate([mod_y[k, 1:2] for k in range(NY)], axis=1)
    gate_s[...] = jnp.concatenate([mod_y[k, 2:3] for k in range(NY)], axis=1)
    bias_s[...] = jnp.concatenate([mod_y[k, 3:4, 0:128] for k in range(NY)], axis=0)
    normed = (scaled * (1.0 + scale) + shift).astype(BF16)
    for copy in fetches[13:16]:
        copy.wait()

    def rms(a, g):
        return a * lax.rsqrt(jnp.mean(a * a, axis=-1, keepdims=True) + EPS) * g

    low = rms(dot(normed, dl[...]), lg[...]).astype(BF16)
    u = dot_nt(normed, dr[...])
    turned = jnp.concatenate([-u[:, 16:32], u[:, 0:16], -u[:, 48:64], u[:, 32:48]], axis=1)
    rope = (u * own_table[:, :64] + turned * own_table[:, 64:]).astype(BF16)
    kblk[...] = jnp.concatenate([low, rope, jnp.zeros((ROWS, 64), BF16)], axis=1)
    zk[z, x] = kblk[...]
    kcopies = [remote(kblk, zk.at[z, x], ks.at[d], kr.at[d], x=xp[d]) for d in range(1, NX)]

    def slot_of(offset):
        return lax.rem(z + offset + NZ, NZ)

    def piece(offset, j):
        return zk.at[slot_of(offset), lax.rem(x - piece_order(j) + NX, NX)]

    def go_right(s, j):
        return remote(piece(1 - s, j), piece(1 - s, j), rs.at[s, j], rr.at[s, j], z=right)

    def go_left(s, j):
        return remote(piece(s - 1, j), piece(s - 1, j), ls.at[s, j], lr.at[s, j], z=left)

    for copy in kcopies:
        copy.start()
    go_right(1, 0).start()
    go_left(1, 0).start()
    qlow[...] = rms(dot(normed, dq[...]), qg[...]).astype(BF16)
    qcopies = [remote(qlow, qa.at[y], qs.at[d], qr.at[d], y=yp[d]) for d in range(1, NY)]
    for copy in qcopies:
        copy.start()
    qa[y] = qlow[...]

    before[2].wait_recv()
    hops[2].start()
    across(yp[1], 1, 2).start()
    after[2].wait_recv()
    across(yp[3], 0, 2).start()
    for i in range(3):
        hops[i].wait_recv()
        across(yp[2], 2, i).start()
    for j, d in ((1, 1), (2, 3), (3, 2)):
        kcopies[d - 1].wait_recv()
        go_right(1, j).start()
        go_left(1, j).start()
    for d, slot in ((0, yp[3]), (1, yp[1]), (2, yp[2])):
        for i in range(3):
            across(slot, d, i).wait_recv()
        wq_t[slot] = uq[slot].T
        wv_t[slot] = uv[slot].T
    for k in range(2):
        @pl.when(z != 2 * y + k)
        def _():
            remote(cx, ctx.at[pl.ds(k * NX, NX)], czs.at[0], czr.at[k], z=zp[1]).wait_recv()

    for copy in qcopies:
        copy.wait_recv()

    @pl.loop(0, NY)
    def _(k):
        qt = dot_nt(wq_t[k], qa[...].reshape(QN, 512))
        for h in range(2):
            b = 192 * h
            u = qt[b + 128 : b + 192]
            turned = jnp.concatenate([-u[16:32], u[0:16], -u[48:64], u[32:48]], axis=0)
            rope = u * line_t[:64] + turned * line_t[64:]
            q_t[k, h] = jnp.concatenate(
                [qt[b : b + 128], rope, jnp.zeros((64, QN), F32)], axis=0
            ).astype(BF16)

    def softmax(s_ref, n, k, h, biased):
        top = jnp.max(s_ref[0:n], axis=0, keepdims=True) * SCALE2
        lift = bias_s[pl.ds(k, 1), h : h + 1] * LOG2E if biased else None
        m_old = m_s[k, h]
        m_new = jnp.maximum(m_old, top + lift if biased else top)
        p = jnp.exp2(s_ref[0:n] * SCALE2 - (m_new - lift if biased else m_new))
        shrink = jnp.exp2(m_old - m_new)
        l_s[k, h] = l_s[k, h] * shrink + jnp.sum(p, axis=0, keepdims=True)
        m_s[k, h] = m_new
        return p.astype(BF16), shrink

    def process(n, load, biased, hook, finish=None):
        def project(k):
            low = load()[:, :256]
            return dot(low, uk[k]).astype(BF16), dot_nt(wv_t[k], low).astype(BF16)

        def score(nope, h, k):
            key = jnp.concatenate([nope[:, 128 * h : 128 * h + 128], load()[:, 256:]], axis=1)
            return dot(key, q_t[k, h])

        def step(k, final):
            hook(k)
            now = kn[0:n]
            sb[0:n] = score(now, 1, k)
            if not final:
                nope, val = project(k + 1)
            p, shrink = softmax(sa, n, k, 0, biased)
            acc[k, 0] = acc[k, 0] * shrink + dot(vt[0:128, 0:n], p)
            if not final:
                sa[0:n] = score(nope, 0, k + 1)
            p, shrink = softmax(sb, n, k, 1, biased)
            acc[k, 1] = acc[k, 1] * shrink + dot(vt[128:256, 0:n], p)
            if not final:
                kn[0:n] = nope
                vt[:, 0:n] = val
            if finish is not None:
                finish(k)

        nope, val = project(0)
        kn[0:n] = nope
        vt[:, 0:n] = val
        sa[0:n] = score(nope, 0, 0)

        @pl.loop(0, NY - 1)
        def _(k):
            step(k, False)

        step(NY - 1, True)

    def nothing(k):
        pass

    def pass_on(s):
        def hook(k):
            go_right(s, k).wait_recv()
            go_left(s, k).wait_recv()
            go_right(s + 1, k).start()
            go_left(s + 1, k).start()

        return hook

    def pass_last(k):
        go_right(3, k).wait_recv()
        go_left(3, k).wait_recv()

        @pl.when(k < 2)
        def _():
            go_right(4, k).start()

        @pl.when(k >= 2)
        def _():
            go_left(4, k).start()

    def bundle(offset):
        return zk[slot_of(offset)].reshape(BUNDLE, 384)

    def around(s):
        return lambda: jnp.concatenate([bundle(-s), bundle(s)], axis=0)

    def out_copy(k, d):
        return remote(ob.at[k, yp[d]], rb.at[d, k], os.at[d, k], orr.at[d, k], y=yp[d])

    def finish(k):
        both = []
        for h in range(2):
            total = l_s[k, h]
            both.append((acc[k, h] / total).T)
            row = m_s[k, h] + jnp.log2(total)
            for j in range(NY):
                st[j, k, h : h + 1] = jnp.concatenate(
                    [row[:, ROWS * j : ROWS * j + ROWS], jnp.zeros((1, 32), F32)], axis=1
                )
        ob[k] = jnp.concatenate(both, axis=1).astype(BF16).reshape(NY, ROWS, 256)
        for d in range(1, NY):
            out_copy(k, d).start()

    process(CTXK, lambda: ctx[...].reshape(CTXK, 384), True, nothing)
    process(BUNDLE, lambda: bundle(0), False, pass_on(1))
    process(2 * BUNDLE, around(1), False, pass_on(2))
    process(2 * BUNDLE, around(2), False, pass_last)
    for j in range(2):
        go_right(4, j).wait_recv()
        go_left(4, j + 2).wait_recv()
    process(
        3 * BUNDLE,
        lambda: jnp.concatenate([bundle(-3), bundle(3), bundle(4)], axis=0),
        False, nothing, finish,
    )

    def stat_copy(d):
        return remote(st.at[yp[d]], rst.at[d], ss.at[d], sr.at[d], y=yp[d])

    for d in range(1, NY):
        stat_copy(d).start()
    for d in range(1, NY):
        stat_copy(d).wait_recv()
    stats = [st[y]] + [rst[d] for d in range(1, NY)]
    top = jnp.maximum(jnp.maximum(stats[0], stats[1]), jnp.maximum(stats[2], stats[3]))
    raised = [jnp.exp2(s - top) for s in stats]
    whole = raised[0] + raised[1] + raised[2] + raised[3]
    fill = jnp.zeros((120, 128), F32)
    shares = [
        jnp.concatenate([(r / whole).reshape(8, 128), fill], axis=0).T[:ROWS] for r in raised
    ]
    fetches[16].wait()
    for k in range(NY):
        for d in range(1, NY):
            out_copy(k, d).wait_recv()
        pieces = [ob[k, y]] + [rb[d, k] for d in range(1, NY)]
        both = []
        for h in range(2):
            head = 2 * k + h
            both.append(sum(
                p[:, 128 * h : 128 * h + 128].astype(F32) * share[:, head : head + 1]
                for p, share in zip(pieces, shares)
            ))
        part = dot(jnp.concatenate(both, axis=1).astype(BF16), ow[256 * k : 256 * k + 256])
        if k == 0:
            mixed[...] = part
        elif k < NY - 1:
            mixed[...] += part
        else:
            out[...] = (
                lat[...].astype(F32) + gate_s[...] * (mixed[...] + part)
            ).astype(BF16)

    for copy in xcopies + ccopies + zcopies + ycopies + after + before + hops + kcopies + qcopies:
        copy.wait_send()

    @pl.when(mine)
    def _():
        for copy in zc:
            copy.wait_send()

    for d in range(3):
        for i in range(3):
            across(yp[d], d, i).wait_send()
    for j in range(NX):
        for s in range(1, 4):
            go_right(s, j).wait_send()
            go_left(s, j).wait_send()
        if j < 2:
            go_right(4, j).wait_send()
        else:
            go_left(4, j).wait_send()
    for d in range(1, NY):
        stat_copy(d).wait_send()
        for k in range(NY):
            out_copy(k, d).wait_send()


def rope_constants():
    inverse = (10000.0 ** (-np.arange(16, dtype=np.float64) / 16)).astype(np.float32)

    def spread(count, first):
        angles = (np.arange(count, dtype=np.float32)[:, None] * inverse).astype(np.float64)
        zero = np.zeros((count, 32))
        runs = []
        for f in (np.cos, np.sin):
            pair = np.concatenate([f(angles), f(angles)], axis=1)
            runs += [pair, zero] if first else [zero, pair]
        return np.concatenate(runs, axis=1).astype(np.float32)

    return spread(192, True), spread(GRID_W, False)


def on_device(
    latent_in, condition, context_latent, context_rope, shift_weight, scale_weight, gate_weight,
    norm_gain, down_query, down_latent, down_rope, query_gain, latent_gain, up_query, up_key,
    up_value, context_bias, out_weight,
):
    row_table, col_table = rope_constants()
    vmem = pltpu.VMEM
    dma = pltpu.SemaphoreType.DMA
    return pl.pallas_call(
        kernel,
        name="whole",
        out_shape=jax.ShapeDtypeStruct((ROWS, D), BF16),
        in_specs=[pl.BlockSpec(memory_space=pltpu.HBM)] * 20,
        out_specs=pl.BlockSpec(memory_space=pltpu.VMEM),
        scratch_shapes=[
            vmem((1, 64), BF16),
            vmem((64, 512), BF16), vmem((64, 512), BF16), vmem((64, 512), BF16),
            vmem((1, 2), F32),
            vmem((ROWS, D), BF16),
            vmem((1, D), F32), vmem((1, 512), F32), vmem((1, 256), F32),
            vmem((192, 128), F32), vmem((GRID_W, 128), F32),
            vmem((16, 256), BF16), vmem((16, 64), BF16),
            vmem((D, 512), BF16), vmem((D, 256), BF16), vmem((64, D), BF16),
            vmem((1024, D), BF16),
            vmem((NY, 512, 384), BF16), vmem((NY, 256, 256), BF16), vmem((NY, 256, 256), BF16),
            vmem((NX, 3, 512), F32), vmem((NZ, 3, 512), F32), vmem((NY, 4, 512), F32),
            vmem((16, 384), BF16), vmem((NX, 16, 384), BF16), vmem((8, 16, 384), BF16),
            vmem((ROWS, 384), BF16), vmem((ROWS, 512), BF16),
            vmem((1, D), F32), vmem((NY, 128), F32),
            vmem((NY, ROWS, 512), BF16),
            vmem((NZ, NX, ROWS, 384), BF16),
            vmem((NY, 384, 512), BF16), vmem((NY, 256, 256), BF16),
            vmem((NY, 2, 256, QN), BF16),
            vmem((3 * BUNDLE, 256), BF16), vmem((256, 3 * BUNDLE), BF16),
            vmem((3 * BUNDLE, QN), F32), vmem((3 * BUNDLE, QN), F32),
            vmem((NY, 2, 1, QN), F32), vmem((NY, 2, 1, QN), F32),
            vmem((NY, 2, 128, QN), F32),
            vmem((NY, NY, ROWS, 256), BF16), vmem((NY, NY, ROWS, 256), BF16),
            vmem((NY, NY, 2, 128), F32), vmem((NY, NY, 2, 128), F32),
            vmem((ROWS, D), F32),
            dma((17,)), dma((3,)),
            dma((NX,)), dma((NX,)),
            dma((NZ,)), dma((NZ,)),
            dma((NY,)), dma((NY,)),
            dma((NX,)), dma((NX,)),
            dma((NZ,)), dma((2,)),
            dma((2, 3)), dma((2, 3)),
            dma((3,)), dma((3,)),
            dma((3, 3)), dma((3, 3)),
            dma((NX,)), dma((NX,)),
            dma((NY,)), dma((NY,)),
            dma((5, NX)), dma((5, NX)),
            dma((5, NX)), dma((5, NX)),
            dma((NY, NY)), dma((NY, NY)),
            dma((NY,)), dma((NY,)),
        ],
        compiler_params=pltpu.CompilerParams(
            collective_id=0, has_side_effects=True, vmem_limit_bytes=60 * 1024 * 1024
        ),
    )(
        condition.reshape(1, -1), shift_weight, scale_weight, gate_weight,
        context_bias.reshape(1, -1), latent_in, norm_gain.reshape(1, -1),
        query_gain.reshape(1, -1), latent_gain.reshape(1, -1), jnp.asarray(row_table),
        jnp.asarray(col_table), context_latent, context_rope, down_query, down_latent,
        down_rope.T, up_query, up_key, up_value, out_weight,
    )


def solution(mesh):
    split = Mesh(mesh.devices.reshape(NZ, NX, NY, 2), ("z", "x", "y", "c"))
    rows = P(("c", "z", "x", "y"), None)
    held = P(("c", "z", "x"), None)
    weight = P(("z", "x"), "y")
    placed = (
        rows, P(("c", "z", "x")), held, held, weight, weight, weight, P(), P(), P(), P(), P(),
        P(), P(None, "y"), P(None, "y"), P(None, "y"), P("y"), P(),
    )
    return jax.shard_map(
        on_device, mesh=split, in_specs=placed, out_specs=rows, check_vma=False
    )
```

```python
import math

import jax
import jax.numpy as jnp
import numpy as np
from jax import lax
from jax.experimental import pallas as pl
from jax.experimental.pallas import tpu as pltpu
from jax.sharding import Mesh
from jax.sharding import PartitionSpec as P

ROWS = 96
D = 2048
NZ, NX, NY = 8, 4, 4
GRID_W = 64
CTXK = 128
EPS = 1e-06
QN = NY * ROWS
ROWS_A, ROWS_B = 64, 32
PIECE_A, PIECE_B = ROWS_A + 16, ROWS_B + 16
BUNDLE = NX * ROWS_A
LAST = 3 * BUNDLE + (NX - 1) * NZ * ROWS_B
LOG2E = math.log2(math.e)
SCALE2 = LOG2E / math.sqrt(192.0)
MESH = pl.DeviceIdType.MESH
F32 = jnp.float32
BF16 = jnp.bfloat16
NEG = float("-inf")


def dot(a, b):
    return jnp.dot(a, b, preferred_element_type=F32)


def dot_nt(a, b):
    return lax.dot_general(a, b, (((1,), (1,)), ((), ())), preferred_element_type=F32)


def remote(src, dst, send_sem, recv_sem, **where):
    return pltpu.make_async_remote_copy(
        src_ref=src, dst_ref=dst, send_sem=send_sem, recv_sem=recv_sem,
        device_id=where, device_id_type=MESH,
    )


def lane_pair(run):
    return jnp.concatenate([run[:, 64:], run[:, :64]], axis=1)


def piece_order(k):
    return k + (k // 2) * (5 - 2 * k)


def kernel(
    cond_h, sw_h, cw_h, gw_h, bias_h, lat_h, gain_h, qg_h, lg_h, rowt_h, colt_h, ctxl_h, ctxr_h,
    dq_h, dl_h, dr_h, uq_h, uk_h, uv_h, ow_h,
    out,
    cond, sw, cw, gw, bias, lat, gain, qg, lg, rowt, colt, ctxl, ctxr, dq, dl, dr, ow,
    uq, uk, uv, mod_x, mod_z, mod_y, cblk, cx, ctx, qlow, gate_s, bias_s,
    qa, zka, zkb, wq_t, wv_t, q_t, lows, ropes, kn, vt, sa, sb, m_s, l_s, acc, ob, rb, st, rst, mixed,
    in_sem, own_sem, xs, xr, zs, zr, ys, yr, cxs, cxr, czs, czr, ws, wr, hs, hr, es, er, fs, fr,
    ks, kr, bs, br, js, jr, qs, qr, rs, rr, ls, lr, os, orr, ss, sr,
):
    z, x, y, c = (lax.axis_index(n) for n in ("z", "x", "y", "c"))
    sp = z * NX + x
    fetches = [
        pltpu.make_async_copy(h, v, in_sem.at[i])
        for i, (h, v) in enumerate((
            (cond_h, cond), (sw_h, sw), (cw_h, cw), (gw_h, gw), (bias_h, bias), (ctxl_h, ctxl),
            (ctxr_h, ctxr), (lat_h, lat), (gain_h, gain), (qg_h, qg), (lg_h, lg),
            (rowt_h, rowt), (colt_h, colt), (dq_h, dq), (dl_h, dl), (dr_h, dr), (ow_h, ow),
        ))
    ]
    owns = [
        pltpu.make_async_copy(h, v.at[y], own_sem.at[i])
        for i, (h, v) in enumerate(((uq_h, uq), (uk_h, uk), (uv_h, uv)))
    ]
    for copy in fetches[:8] + owns + fetches[8:]:
        copy.start()
    xp = [lax.rem(x + d, NX) for d in range(NX)]
    yp = [lax.rem(y + d, NY) for d in range(NY)]
    zp = [lax.rem(z + d, NZ) for d in range(NZ)]
    right, left = zp[1], zp[NZ - 1]
    peers = (
        [{"x": xp[d]} for d in range(1, NX)]
        + [{"y": yp[d]} for d in range(1, NY)]
        + [{"z": zp[d]} for d in range(1, NZ)]
        + [{"c": 1 - c}]
    )
    barrier = pltpu.get_barrier_semaphore()
    for where in peers:
        pl.semaphore_signal(barrier, inc=1, device_id=where, device_id_type=MESH)

    for copy in fetches[:7]:
        copy.wait()
    v = cond[...].astype(F32)
    activated = (v / (1.0 + jnp.exp(-v))).astype(BF16)
    mod_x[x] = jnp.concatenate([dot(activated, w[...]) for w in (sw, cw, gw)], axis=0)
    for copy in owns:
        copy.wait()
    pl.semaphore_wait(barrier, len(peers))
    xcopies = [
        remote(mod_x.at[x], mod_x.at[x], xs.at[d], xr.at[d], x=xp[d]) for d in range(1, NX)
    ]
    for copy in xcopies:
        copy.start()
    cblk[...] = jnp.concatenate([ctxl[...], ctxr[...], jnp.zeros((16, 64), BF16)], axis=1)
    cx[x] = cblk[...]
    ccopies = [remote(cblk, cx.at[x], cxs.at[d], cxr.at[d], x=xp[d]) for d in range(1, NX)]
    for copy in ccopies:
        copy.start()

    def half(ref, slot):
        rows = ref.shape[1] // 2
        return ref.at[slot, pl.ds(pl.multiple_of(c * rows, rows), rows)]

    def eighth(slot):
        return uq.at[slot, pl.ds(pl.multiple_of(c * 256 + x * 64, 64), 64)]

    def over_y(d, i):
        return remote(half(ups[i], y), half(ups[i], y), ws.at[d, i], wr.at[d, i], y=yp[d])

    def eighth_over_y(d):
        return remote(eighth(y), eighth(y), hs.at[d], hr.at[d], y=yp[d])

    def eighth_over_x(d, e):
        slot = yp[NY - d]
        return remote(eighth(slot), eighth(slot), es.at[d, e], er.at[d, e], x=xp[e])

    def across(d, i):
        slot = yp[NY - d]
        return remote(half(ups[i], slot), half(ups[i], slot), fs.at[d, i], fr.at[d, i], c=1 - c)

    ups = (uq, uk, uv)
    nearest = (1, 3, 2)
    for d in nearest:
        eighth_over_y(d).start()
    for i in (1, 2):
        for d in nearest:
            over_y(d, i).start()

    for copy in xcopies:
        copy.wait_recv()
    mod_z[z] = mod_x[0] + mod_x[1] + mod_x[2] + mod_x[3]
    zcopies = [
        remote(mod_z.at[z], mod_z.at[z], zs.at[d], zr.at[d], z=zp[d]) for d in range(1, NZ)
    ]
    for copy in zcopies:
        copy.start()
    for copy in fetches[7:13]:
        copy.wait()
    lat32 = lat[...].astype(F32)
    inv = lax.rsqrt(jnp.mean(lat32 * lat32, axis=-1, keepdims=True) + EPS)
    scaled = lat32 * inv * gain[...]
    line = [rowt[pl.ds(sp * 6 + i, 1), :] + colt[...] for i in range(6)]
    line_t = jnp.concatenate(line, axis=0).T
    own_table = []
    for t in range(3):
        g = y * 3 + t
        own_table.append(
            rowt[pl.ds(sp * 6 + g // 2, 1), :]
            + colt[pl.ds(pl.multiple_of((g % 2) * 32, 32), 32), :]
        )
    own_table = jnp.concatenate(own_table, axis=0)
    wq_t[y] = uq[y].T
    wv_t[y] = uv[y].T
    m_s[...] = jnp.full(m_s.shape, NEG, F32)
    l_s[...] = jnp.zeros(l_s.shape, F32)
    acc[...] = jnp.zeros(acc.shape, F32)
    for copy in ccopies:
        copy.wait_recv()
    mine = z // 2 == y
    zc = [
        remote(
            cx, ctx.at[pl.ds(pl.multiple_of((z % 2) * NX, NX), NX)], czs.at[d],
            czr.at[z % 2], z=zp[d],
        )
        for d in range(1, NZ)
    ]

    @pl.when(mine)
    def _():
        ctx[pl.ds((z % 2) * NX, NX)] = cx[...]
        for copy in zc:
            copy.start()

    for d in nearest:
        eighth_over_y(d).wait_recv()
        for e in nearest:
            eighth_over_x(d, e).start()

    for copy in zcopies:
        copy.wait_recv()
    total = mod_z[0]
    for k in range(1, NZ):
        total = total + mod_z[k]
    bias_row = jnp.concatenate([bias[...], jnp.zeros((1, 510), F32)], axis=1)
    mod_y[y] = jnp.concatenate([total, bias_row], axis=0)
    ycopies = [
        remote(mod_y.at[y], mod_y.at[y], ys.at[d], yr.at[d], y=yp[d]) for d in range(1, NY)
    ]
    for copy in ycopies:
        copy.start()
    for i in (1, 2):
        for d in nearest:
            over_y(d, i).wait_recv()
            across(d, i).start()

    for copy in ycopies:
        copy.wait_recv()
    shift = jnp.concatenate([mod_y[k, 0:1] for k in range(NY)], axis=1)
    scale = jnp.concatenate([mod_y[k, 1:2] for k in range(NY)], axis=1)
    gate_s[...] = jnp.concatenate([mod_y[k, 2:3] for k in range(NY)], axis=1)
    bias_s[...] = jnp.concatenate([mod_y[k, 3:4, 0:128] for k in range(NY)], axis=0)
    normed = (scaled * (1.0 + scale) + shift).astype(BF16)
    for copy in fetches[13:16]:
        copy.wait()

    def rms(a, g):
        return a * lax.rsqrt(jnp.mean(a * a, axis=-1, keepdims=True) + EPS) * g

    qlow[...] = rms(dot(normed, dq[...]), qg[...]).astype(BF16)
    qcopies = [remote(qlow, qa.at[y], qs.at[d], qr.at[d], y=yp[d]) for d in range(1, NY)]
    for copy in qcopies:
        copy.start()
    low = rms(dot(normed, dl[...]), lg[...]).astype(BF16)
    u = dot_nt(normed, dr[...])
    turned = jnp.concatenate([-u[:, 16:32], u[:, 0:16], -u[:, 48:64], u[:, 32:48]], axis=1)
    rope = u * own_table[:, :64] + turned * own_table[:, 64:]
    runs = [rope[16 * g : 16 * g + 16] for g in range(6)]
    zka[z, x] = jnp.concatenate(
        [low[:ROWS_A], jnp.concatenate(runs[:4], axis=1).astype(BF16)], axis=0
    )
    zkb[x, z] = jnp.concatenate(
        [
            low[ROWS_A:],
            jnp.concatenate(runs[4:] + [jnp.zeros((16, 128), F32)], axis=1).astype(BF16),
        ],
        axis=0,
    )

    def slot_of(offset):
        return lax.rem(z + offset + NZ, NZ)

    def piece(offset, j):
        return zka.at[slot_of(offset), lax.rem(x - piece_order(j) + NX, NX)]

    def go_right(s, j):
        return remote(piece(1 - s, j), piece(1 - s, j), rs.at[s, j], rr.at[s, j], z=right)

    def go_left(s, j):
        return remote(piece(s - 1, j), piece(s - 1, j), ls.at[s, j], lr.at[s, j], z=left)

    kcopies = [
        remote(zka.at[z, x], zka.at[z, x], ks.at[d], kr.at[d], x=xp[d]) for d in range(1, NX)
    ]
    bcopies = [
        remote(zkb.at[x, z], zkb.at[x, z], bs.at[d], br.at[d], z=zp[d]) for d in range(1, NZ)
    ]
    lines = [remote(zkb.at[x], zkb.at[x], js.at[d], jr.at[d], x=xp[d]) for d in range(1, NX)]
    for copy in kcopies:
        copy.start()
    go_right(1, 0).start()
    go_left(1, 0).start()
    for copy in bcopies:
        copy.start()
    qa[y] = qlow[...]

    for d in nearest:
        for e in nearest:
            eighth_over_x(d, e).wait_recv()
        across(d, 0).start()
    for j, d in ((1, 1), (2, 3), (3, 2)):
        kcopies[d - 1].wait_recv()
        go_right(1, j).start()
        go_left(1, j).start()
    for d in nearest:
        for i in (1, 2, 0):
            across(d, i).wait_recv()
        slot = yp[NY - d]
        wq_t[slot] = uq[slot].T
        wv_t[slot] = uv[slot].T
    for k in range(2):
        @pl.when(z != 2 * y + k)
        def _():
            remote(cx, ctx.at[pl.ds(k * NX, NX)], czs.at[0], czr.at[k], z=zp[1]).wait_recv()

    for copy in qcopies:
        copy.wait_recv()

    @pl.loop(0, NY)
    def _(k):
        qt = dot_nt(wq_t[k], qa[...].reshape(QN, 512))
        for h in range(2):
            b = 192 * h
            u = qt[b + 128 : b + 192]
            turned = jnp.concatenate([-u[16:32], u[0:16], -u[48:64], u[32:48]], axis=0)
            rope = u * line_t[:64] + turned * line_t[64:]
            q_t[k, h] = jnp.concatenate(
                [qt[b : b + 128], rope, jnp.zeros((64, QN), F32)], axis=0
            ).astype(BF16)

    def softmax(s_ref, n, k, h, biased):
        top = jnp.max(s_ref[0:n], axis=0, keepdims=True) * SCALE2
        lift = bias_s[pl.ds(k, 1), h : h + 1] * LOG2E if biased else None
        m_old = m_s[k, h]
        m_new = jnp.maximum(m_old, top + lift if biased else top)
        p = jnp.exp2(s_ref[0:n] * SCALE2 - (m_new - lift if biased else m_new))
        shrink = jnp.exp2(m_old - m_new)
        l_s[k, h] = l_s[k, h] * shrink + jnp.sum(p, axis=0, keepdims=True)
        m_s[k, h] = m_new
        return p.astype(BF16), shrink

    def pass_on(s, j):
        go_right(s, j).wait_recv()
        go_left(s, j).wait_recv()
        if s < 3 or j < 2:
            go_right(s + 1, j).start()
        if s < 3 or j >= 2:
            go_left(s + 1, j).start()

    def process(n, stage, biased, passes, finish=None):
        def project(k):
            return dot(lows[0:n], uk[k]).astype(BF16), dot_nt(wv_t[k], lows[0:n]).astype(BF16)

        def score(nope, h, k):
            key = jnp.concatenate([nope[:, 128 * h : 128 * h + 128], ropes[0:n]], axis=1)
            return dot(key, q_t[k, h])

        def step(k, final):
            for at, s, j in passes:
                if final and at == NY - 1:
                    pass_on(s, j)
                elif not final and at < NY - 1:
                    pl.when(k == at)(lambda s=s, j=j: pass_on(s, j))
            now = kn[0:n]
            sb[0:n] = score(now, 1, k)
            if not final:
                nope, val = project(k + 1)
            p, shrink = softmax(sa, n, k, 0, biased)
            acc[k, 0] = acc[k, 0] * shrink + dot(vt[0:128, 0:n], p)
            if not final:
                sa[0:n] = score(nope, 0, k + 1)
            p, shrink = softmax(sb, n, k, 1, biased)
            acc[k, 1] = acc[k, 1] * shrink + dot(vt[128:256, 0:n], p)
            if not final:
                kn[0:n] = nope
                vt[:, 0:n] = val
            if finish is not None:
                finish(k)

        stage()
        nope, val = project(0)
        kn[0:n] = nope
        vt[:, 0:n] = val
        sa[0:n] = score(nope, 0, 0)

        @pl.loop(0, NY - 1)
        def _(k):
            step(k, False)

        step(NY - 1, True)

    def stage_context():
        both = ctx[...].reshape(CTXK, 384)
        lows[0:CTXK] = both[:, :256]
        ropes[0:CTXK] = both[:, 256:]

    def stage_a(at, offset):
        slot = slot_of(offset)
        lows[at : at + BUNDLE] = zka[slot, :, :ROWS_A].reshape(BUNDLE, 256)
        for i in range(NX):
            run = zka[slot, i, ROWS_A:]
            for g in range(4):
                tile = run[:, 128 * (g // 2) : 128 * (g // 2) + 128]
                first = at + ROWS_A * i + 16 * g
                ropes[first : first + 16] = lane_pair(tile) if g % 2 else tile

    def stage_b(at, line):
        lows[at : at + NZ * ROWS_B] = zkb[line, :, :ROWS_B].reshape(NZ * ROWS_B, 256)
        for i in range(NZ):
            tile = zkb[line, i, ROWS_B:, :128]
            first = at + ROWS_B * i
            ropes[first : first + 16] = tile
            ropes[first + 16 : first + 32] = lane_pair(tile)

    def out_copy(k, d):
        return remote(ob.at[k, yp[d]], rb.at[d, k], os.at[d, k], orr.at[d, k], y=yp[d])

    def finish(k):
        both = []
        for h in range(2):
            total = l_s[k, h]
            both.append((acc[k, h] / total).T)
            row = m_s[k, h] + jnp.log2(total)
            for j in range(NY):
                st[j, k, h : h + 1] = jnp.concatenate(
                    [row[:, ROWS * j : ROWS * j + ROWS], jnp.zeros((1, 32), F32)], axis=1
                )
        ob[k] = jnp.concatenate(both, axis=1).astype(BF16).reshape(NY, ROWS, 256)
        for d in range(1, NY):
            out_copy(k, d).start()

    def stage_own():
        stage_a(0, 0)
        stage_b(BUNDLE, x)

    def stage_around(s):
        def stage():
            stage_a(0, -s)
            stage_a(BUNDLE, s)

        return stage

    def stage_last():
        for i, offset in enumerate((-3, 3, 4)):
            stage_a(i * BUNDLE, offset)
        for d in range(1, NX):
            stage_b((2 + d) * BUNDLE, xp[NX - d])

    pass_on(1, 0)
    process(CTXK, stage_context, True, ((2, 1, 1), (3, 1, 2)))
    for copy in bcopies:
        copy.wait_recv()
    for copy in lines:
        copy.start()
    process(2 * BUNDLE, stage_own, False, ((0, 1, 3), (2, 2, 0), (3, 2, 1)))
    process(2 * BUNDLE, stage_around(1), False, ((0, 2, 2), (1, 2, 3), (3, 3, 0)))
    process(2 * BUNDLE, stage_around(2), False, ((0, 3, 1), (1, 3, 2), (2, 3, 3)))
    for j in range(2):
        go_right(4, j).wait_recv()
        go_left(4, j + 2).wait_recv()
    for copy in lines:
        copy.wait_recv()
    process(LAST, stage_last, False, (), finish)

    def stat_copy(d):
        return remote(st.at[yp[d]], rst.at[d], ss.at[d], sr.at[d], y=yp[d])

    for d in range(1, NY):
        stat_copy(d).start()
    for d in range(1, NY):
        stat_copy(d).wait_recv()
    stats = [st[y]] + [rst[d] for d in range(1, NY)]
    top = jnp.maximum(jnp.maximum(stats[0], stats[1]), jnp.maximum(stats[2], stats[3]))
    raised = [jnp.exp2(s - top) for s in stats]
    whole = raised[0] + raised[1] + raised[2] + raised[3]
    fill = jnp.zeros((120, 128), F32)
    shares = [
        jnp.concatenate([(r / whole).reshape(8, 128), fill], axis=0).T[:ROWS] for r in raised
    ]
    fetches[16].wait()
    for k in range(NY):
        for d in range(1, NY):
            out_copy(k, d).wait_recv()
        pieces = [ob[k, y]] + [rb[d, k] for d in range(1, NY)]
        both = []
        for h in range(2):
            head = 2 * k + h
            both.append(sum(
                p[:, 128 * h : 128 * h + 128].astype(F32) * share[:, head : head + 1]
                for p, share in zip(pieces, shares)
            ))
        part = dot(jnp.concatenate(both, axis=1).astype(BF16), ow[256 * k : 256 * k + 256])
        if k == 0:
            mixed[...] = part
        elif k < NY - 1:
            mixed[...] += part
        else:
            out[...] = (
                lat[...].astype(F32) + gate_s[...] * (mixed[...] + part)
            ).astype(BF16)

    for copy in xcopies + ccopies + zcopies + ycopies + kcopies + qcopies + bcopies + lines:
        copy.wait_send()

    @pl.when(mine)
    def _():
        for copy in zc:
            copy.wait_send()

    for d in nearest:
        eighth_over_y(d).wait_send()
        for i in range(3):
            across(d, i).wait_send()
            if i > 0:
                over_y(d, i).wait_send()
        for e in nearest:
            eighth_over_x(d, e).wait_send()
    for j in range(NX):
        for s in range(1, 4):
            go_right(s, j).wait_send()
            go_left(s, j).wait_send()
        if j < 2:
            go_right(4, j).wait_send()
        else:
            go_left(4, j).wait_send()
    for d in range(1, NY):
        stat_copy(d).wait_send()
        for k in range(NY):
            out_copy(k, d).wait_send()


def rope_constants():
    inverse = (10000.0 ** (-np.arange(16, dtype=np.float64) / 16)).astype(np.float32)

    def spread(count, first):
        angles = (np.arange(count, dtype=np.float32)[:, None] * inverse).astype(np.float64)
        zero = np.zeros((count, 32))
        runs = []
        for f in (np.cos, np.sin):
            pair = np.concatenate([f(angles), f(angles)], axis=1)
            runs += [pair, zero] if first else [zero, pair]
        return np.concatenate(runs, axis=1).astype(np.float32)

    return spread(192, True), spread(GRID_W, False)


def on_device(
    latent_in, condition, context_latent, context_rope, shift_weight, scale_weight, gate_weight,
    norm_gain, down_query, down_latent, down_rope, query_gain, latent_gain, up_query, up_key,
    up_value, context_bias, out_weight,
):
    row_table, col_table = rope_constants()
    vmem = pltpu.VMEM
    dma = pltpu.SemaphoreType.DMA
    return pl.pallas_call(
        kernel,
        name="whole",
        out_shape=jax.ShapeDtypeStruct((ROWS, D), BF16),
        in_specs=[pl.BlockSpec(memory_space=pltpu.HBM)] * 20,
        out_specs=pl.BlockSpec(memory_space=pltpu.VMEM),
        scratch_shapes=[
            vmem((1, 64), BF16),
            vmem((64, 512), BF16), vmem((64, 512), BF16), vmem((64, 512), BF16),
            vmem((1, 2), F32),
            vmem((ROWS, D), BF16),
            vmem((1, D), F32), vmem((1, 512), F32), vmem((1, 256), F32),
            vmem((192, 128), F32), vmem((GRID_W, 128), F32),
            vmem((16, 256), BF16), vmem((16, 64), BF16),
            vmem((D, 512), BF16), vmem((D, 256), BF16), vmem((64, D), BF16),
            vmem((1024, D), BF16),
            vmem((NY, 512, 384), BF16), vmem((NY, 256, 256), BF16), vmem((NY, 256, 256), BF16),
            vmem((NX, 3, 512), F32), vmem((NZ, 3, 512), F32), vmem((NY, 4, 512), F32),
            vmem((16, 384), BF16), vmem((NX, 16, 384), BF16), vmem((8, 16, 384), BF16),
            vmem((ROWS, 512), BF16),
            vmem((1, D), F32), vmem((NY, 128), F32),
            vmem((NY, ROWS, 512), BF16),
            vmem((NZ, NX, PIECE_A, 256), BF16), vmem((NX, NZ, PIECE_B, 256), BF16),
            vmem((NY, 384, 512), BF16), vmem((NY, 256, 256), BF16),
            vmem((NY, 2, 256, QN), BF16),
            vmem((LAST, 256), BF16), vmem((LAST, 128), BF16),
            vmem((LAST, 256), BF16), vmem((256, LAST), BF16),
            vmem((LAST, QN), F32), vmem((LAST, QN), F32),
            vmem((NY, 2, 1, QN), F32), vmem((NY, 2, 1, QN), F32),
            vmem((NY, 2, 128, QN), F32),
            vmem((NY, NY, ROWS, 256), BF16), vmem((NY, NY, ROWS, 256), BF16),
            vmem((NY, NY, 2, 128), F32), vmem((NY, NY, 2, 128), F32),
            vmem((ROWS, D), F32),
            dma((17,)), dma((3,)),
            dma((NX,)), dma((NX,)),
            dma((NZ,)), dma((NZ,)),
            dma((NY,)), dma((NY,)),
            dma((NX,)), dma((NX,)),
            dma((NZ,)), dma((2,)),
            dma((NY, 3)), dma((NY, 3)),
            dma((NY,)), dma((NY,)),
            dma((NY, NX)), dma((NY, NX)),
            dma((NY, 3)), dma((NY, 3)),
            dma((NX,)), dma((NX,)),
            dma((NZ,)), dma((NZ,)),
            dma((NX,)), dma((NX,)),
            dma((NY,)), dma((NY,)),
            dma((5, NX)), dma((5, NX)),
            dma((5, NX)), dma((5, NX)),
            dma((NY, NY)), dma((NY, NY)),
            dma((NY,)), dma((NY,)),
        ],
        compiler_params=pltpu.CompilerParams(
            collective_id=0, has_side_effects=True, vmem_limit_bytes=60 * 1024 * 1024
        ),
    )(
        condition.reshape(1, -1), shift_weight, scale_weight, gate_weight,
        context_bias.reshape(1, -1), latent_in, norm_gain.reshape(1, -1),
        query_gain.reshape(1, -1), latent_gain.reshape(1, -1), jnp.asarray(row_table),
        jnp.asarray(col_table), context_latent, context_rope, down_query, down_latent,
        down_rope.T, up_query, up_key, up_value, out_weight,
    )


def solution(mesh):
    split = Mesh(mesh.devices.reshape(NZ, NX, NY, 2), ("z", "x", "y", "c"))
    rows = P(("c", "z", "x", "y"), None)
    held = P(("c", "z", "x"), None)
    weight = P(("z", "x"), "y")
    placed = (
        rows, P(("c", "z", "x")), held, held, weight, weight, weight, P(), P(), P(), P(), P(),
        P(), P(None, "y"), P(None, "y"), P(None, "y"), P("y"), P(),
    )
    return jax.shard_map(
        on_device, mesh=split, in_specs=placed, out_specs=rows, check_vma=False
    )
```

```python
import math

import jax
import jax.numpy as jnp
import numpy as np
from jax import lax
from jax.experimental import pallas as pl
from jax.experimental.pallas import tpu as pltpu
from jax.sharding import Mesh
from jax.sharding import PartitionSpec as P

ROWS = 96
D = 2048
NZ, NX, NY = 8, 4, 4
GRID_W = 64
CTXK = 128
EPS = 1e-06
QN = NY * ROWS
ROWS_A, ROWS_B = 64, 32
PIECE_A, PIECE_B = ROWS_A + 16, ROWS_B + 16
BUNDLE = NX * ROWS_A
LAST = 3 * BUNDLE + (NX - 1) * NZ * ROWS_B
LOG2E = math.log2(math.e)
SCALE2 = LOG2E / math.sqrt(192.0)
MESH = pl.DeviceIdType.MESH
F32 = jnp.float32
BF16 = jnp.bfloat16
NEG = float("-inf")


def dot(a, b):
    return jnp.dot(a, b, preferred_element_type=F32)


def dot_nt(a, b):
    return lax.dot_general(a, b, (((1,), (1,)), ((), ())), preferred_element_type=F32)


def remote(src, dst, send_sem, recv_sem, **where):
    return pltpu.make_async_remote_copy(
        src_ref=src, dst_ref=dst, send_sem=send_sem, recv_sem=recv_sem,
        device_id=where, device_id_type=MESH,
    )


def lane_pair(run):
    return jnp.concatenate([run[:, 64:], run[:, :64]], axis=1)


def piece_order(k):
    return k + (k // 2) * (5 - 2 * k)


def kernel(
    cond_h, sw_h, cw_h, gw_h, bias_h, lat_h, gain_h, qg_h, lg_h, rowt_h, colt_h, ctxl_h, ctxr_h,
    dq_h, dl_h, dr_h, uq_h, uk_h, uv_h, ow_h,
    out,
    cond, sw, cw, gw, bias, lat, gain, qg, lg, rowt, colt, ctxl, ctxr, dq, dl, dr, ow,
    uq, uk, uv, mod_x, mod_z, mod_y, cblk, cx, ctx, qlow, gate_s, bias_s,
    qa, zka, zkb, wq_t, wv_t, q_t, lows, ropes, kn, vt, sa, sb, m_s, l_s, acc, ob, rb, st, rst, mixed,
    in_sem, own_sem, snd, rcv,
):
    z, x, y, c = (lax.axis_index(n) for n in ("z", "x", "y", "c"))
    sp = z * NX + x

    def drain(ref, i):
        remote(ref, ref, snd.at[i], rcv.at[0], c=1 - c).wait_send()

    def landed(ref, i):
        remote(ref, ref, snd.at[0], rcv.at[i], c=1 - c).wait_recv()

    fetches = [
        pltpu.make_async_copy(h, v, in_sem.at[i])
        for i, (h, v) in enumerate((
            (cond_h, cond), (sw_h, sw), (cw_h, cw), (gw_h, gw), (bias_h, bias), (ctxl_h, ctxl),
            (ctxr_h, ctxr), (lat_h, lat), (gain_h, gain), (qg_h, qg), (lg_h, lg),
            (rowt_h, rowt), (colt_h, colt), (dq_h, dq), (dl_h, dl), (dr_h, dr), (ow_h, ow),
        ))
    ]
    owns = [
        pltpu.make_async_copy(h, v.at[y], own_sem.at[i])
        for i, (h, v) in enumerate(((uq_h, uq), (uk_h, uk), (uv_h, uv)))
    ]
    for copy in fetches[:7] + owns:
        copy.start()
    xp = [lax.rem(x + d, NX) for d in range(NX)]
    yp = [lax.rem(y + d, NY) for d in range(NY)]
    zp = [lax.rem(z + d, NZ) for d in range(NZ)]
    right, left = zp[1], zp[NZ - 1]
    peers = (
        [{"x": xp[d]} for d in range(1, NX)]
        + [{"y": yp[d]} for d in range(1, NY)]
        + [{"z": zp[d]} for d in range(1, NZ)]
        + [{"c": 1 - c}]
    )
    barrier = pltpu.get_barrier_semaphore()
    for where in peers:
        pl.semaphore_signal(barrier, inc=1, device_id=where, device_id_type=MESH)

    for copy in fetches[:7]:
        copy.wait()
    v = cond[...].astype(F32)
    activated = (v / (1.0 + jnp.exp(-v))).astype(BF16)
    mod_x[x] = jnp.concatenate([dot(activated, w[...]) for w in (sw, cw, gw)], axis=0)
    pl.semaphore_wait(barrier, len(peers))
    xcopies = [
        remote(mod_x.at[x], mod_x.at[x], snd.at[0], rcv.at[0], x=xp[d]) for d in range(1, NX)
    ]
    for copy in xcopies:
        copy.start()
    for copy in fetches[7:]:
        copy.start()
    for copy in owns:
        copy.wait()
    cblk[...] = jnp.concatenate([ctxl[...], ctxr[...], jnp.zeros((16, 64), BF16)], axis=1)
    cx[x] = cblk[...]
    ccopies = [remote(cblk, cx.at[x], snd.at[1], rcv.at[1], x=xp[d]) for d in range(1, NX)]
    for copy in ccopies:
        copy.start()

    def half(ref, slot):
        rows = ref.shape[1] // 2
        return ref.at[slot, pl.ds(pl.multiple_of(c * rows, rows), rows)]

    def eighth(slot):
        return uq.at[slot, pl.ds(pl.multiple_of(c * 256 + x * 64, 64), 64)]

    def over_y(d, i):
        return remote(half(ups[i], y), half(ups[i], y), snd.at[5 + i], rcv.at[6 + i], y=yp[d])

    def eighth_over_y(d):
        return remote(eighth(y), eighth(y), snd.at[5], rcv.at[6], y=yp[d])

    def eighth_over_x(d, e):
        slot = yp[NY - d]
        return remote(eighth(slot), eighth(slot), snd.at[8], rcv.at[9], x=xp[e])

    def across(d, i):
        slot = yp[NY - d]
        return remote(half(ups[i], slot), half(ups[i], slot), snd.at[9 + i], rcv.at[10 + i], c=1 - c)

    ups = (uq, uk, uv)
    nearest = (1, 3, 2)
    for d in nearest:
        eighth_over_y(d).start()
    for d in nearest:
        over_y(d, 1).start()

    landed(mod_x.at[0:3], 0)
    mod_z[z] = mod_x[0] + mod_x[1] + mod_x[2] + mod_x[3]
    zcopies = [
        remote(mod_z.at[z], mod_z.at[z], snd.at[2], rcv.at[2], z=zp[d]) for d in range(1, NZ)
    ]
    for copy in zcopies:
        copy.start()
    for copy in fetches[7:13]:
        copy.wait()
    lat32 = lat[...].astype(F32)
    inv = lax.rsqrt(jnp.mean(lat32 * lat32, axis=-1, keepdims=True) + EPS)
    scaled = lat32 * inv * gain[...]
    line = [rowt[pl.ds(sp * 6 + i, 1), :] + colt[...] for i in range(6)]
    line_t = jnp.concatenate(line, axis=0).T
    own_table = []
    for t in range(3):
        g = y * 3 + t
        own_table.append(
            rowt[pl.ds(sp * 6 + g // 2, 1), :]
            + colt[pl.ds(pl.multiple_of((g % 2) * 32, 32), 32), :]
        )
    own_table = jnp.concatenate(own_table, axis=0)
    wq_t[y] = uq[y].T
    wv_t[y] = uv[y].T
    m_s[...] = jnp.full(m_s.shape, NEG, F32)
    l_s[...] = jnp.zeros(l_s.shape, F32)
    acc[...] = jnp.zeros(acc.shape, F32)
    landed(cx.at[0:3], 1)
    mine = z // 2 == y
    zc = [
        remote(
            cx, ctx.at[pl.ds(pl.multiple_of((z % 2) * NX, NX), NX)], snd.at[4],
            rcv.at[4 + z % 2], z=zp[d],
        )
        for d in range(1, NZ)
    ]

    @pl.when(mine)
    def _():
        ctx[pl.ds((z % 2) * NX, NX)] = cx[...]
        for copy in zc:
            copy.start()

    landed(uq.at[0, 0:192], 6)
    for d in nearest:
        for e in nearest:
            eighth_over_x(d, e).start()

    landed(mod_z.at[0:7], 2)
    total = mod_z[0]
    for k in range(1, NZ):
        total = total + mod_z[k]
    bias_row = jnp.concatenate([bias[...], jnp.zeros((1, 510), F32)], axis=1)
    mod_y[y] = jnp.concatenate([total, bias_row], axis=0)
    ycopies = [
        remote(mod_y.at[y], mod_y.at[y], snd.at[3], rcv.at[3], y=yp[d]) for d in range(1, NY)
    ]
    for copy in ycopies:
        copy.start()
    for d in nearest:
        over_y(d, 2).start()
    landed(uk.at[0:3, 0:128], 7)
    for d in nearest:
        across(d, 1).start()

    landed(mod_y.at[0:3], 3)
    landed(uq.at[0:3, 0:192], 9)
    for d in nearest:
        across(d, 0).start()
    shift = jnp.concatenate([mod_y[k, 0:1] for k in range(NY)], axis=1)
    scale = jnp.concatenate([mod_y[k, 1:2] for k in range(NY)], axis=1)
    gate_s[...] = jnp.concatenate([mod_y[k, 2:3] for k in range(NY)], axis=1)
    bias_s[...] = jnp.concatenate([mod_y[k, 3:4, 0:128] for k in range(NY)], axis=0)
    normed = (scaled * (1.0 + scale) + shift).astype(BF16)
    for copy in fetches[13:16]:
        copy.wait()

    def rms(a, g):
        return a * lax.rsqrt(jnp.mean(a * a, axis=-1, keepdims=True) + EPS) * g

    qlow[...] = rms(dot(normed, dq[...]), qg[...]).astype(BF16)
    qcopies = [remote(qlow, qa.at[y], snd.at[12], rcv.at[13], y=yp[d]) for d in range(1, NY)]
    for copy in qcopies:
        copy.start()
    low = rms(dot(normed, dl[...]), lg[...]).astype(BF16)
    u = dot_nt(normed, dr[...])
    turned = jnp.concatenate([-u[:, 16:32], u[:, 0:16], -u[:, 48:64], u[:, 32:48]], axis=1)
    rope = u * own_table[:, :64] + turned * own_table[:, 64:]
    runs = [rope[16 * g : 16 * g + 16] for g in range(6)]
    zka[z, x] = jnp.concatenate(
        [low[:ROWS_A], jnp.concatenate(runs[:4], axis=1).astype(BF16)], axis=0
    )
    zkb[x, z] = jnp.concatenate(
        [
            low[ROWS_A:],
            jnp.concatenate(runs[4:] + [jnp.zeros((16, 128), F32)], axis=1).astype(BF16),
        ],
        axis=0,
    )

    def slot_of(offset):
        return lax.rem(z + offset + NZ, NZ)

    def piece(offset, j):
        return zka.at[slot_of(offset), lax.rem(x - piece_order(j) + NX, NX)]

    def turn(s, j):
        return rcv.at[29 if s == 4 else 13 + 4 * s + j]

    def go_right(s, j):
        return remote(piece(1 - s, j), piece(1 - s, j), snd.at[14], turn(s, j), z=right)

    def go_left(s, j):
        return remote(piece(s - 1, j), piece(s - 1, j), snd.at[14], turn(s, j), z=left)

    kcopies = [
        remote(zka.at[z, x], zka.at[z, x], snd.at[13], rcv.at[13 + d], x=xp[d]) for d in range(1, NX)
    ]
    def along_z(origin, d, to):
        held = zkb.at[x, slot_of(origin)]
        group = 30 if d in (2, 6) else 31 if d in (1, 7) else 32
        return remote(held, held, snd.at[15], rcv.at[group], z=to)

    def along_x(o, d):
        held = zkb.at[x, slot_of(-o)]
        return remote(held, held, snd.at[16], rcv.at[33], x=xp[d])

    for copy in kcopies:
        copy.start()
    go_right(1, 0).start()
    go_left(1, 0).start()
    for d in (1, 7, 2, 6):
        along_z(0, d, zp[d]).start()
    for d in nearest:
        along_x(0, d).start()
    qa[y] = qlow[...]

    landed(uv.at[0:3, 0:128], 8)
    for d in nearest:
        across(d, 2).start()
    landed(uq.at[0:3, 0:256], 10)
    for d in nearest:
        slot = yp[NY - d]
        wq_t[slot] = uq[slot].T
    for j, d in ((1, 1), (2, 3), (3, 2)):
        kcopies[d - 1].wait_recv()
        go_right(1, j).start()
        go_left(1, j).start()
    landed(uk.at[0:3, 0:128], 11)
    landed(uv.at[0:3, 0:128], 12)
    for d in nearest:
        slot = yp[NY - d]
        wv_t[slot] = uv[slot].T
    for k in range(2):
        @pl.when(z != 2 * y + k)
        def _():
            landed(ctx.at[pl.ds(k * NX, NX)], 4 + k)

    landed(qa.at[0:3], 13)

    for k in range(NY):
        qt = dot_nt(wq_t[k], qa[...].reshape(QN, 512))
        for h in range(2):
            b = 192 * h
            u = qt[b + 128 : b + 192]
            turned = jnp.concatenate([-u[16:32], u[0:16], -u[48:64], u[32:48]], axis=0)
            rope = u * line_t[:64] + turned * line_t[64:]
            q_t[k, h] = jnp.concatenate(
                [qt[b : b + 128], rope, jnp.zeros((64, QN), F32)], axis=0
            ).astype(BF16)

    def softmax(s_ref, n, k, h, biased):
        top = jnp.max(s_ref[0:n], axis=0, keepdims=True) * SCALE2
        lift = bias_s[pl.ds(k, 1), h : h + 1] * LOG2E if biased else None
        m_old = m_s[k, h]
        m_new = jnp.maximum(m_old, top + lift if biased else top)
        p = jnp.exp2(s_ref[0:n] * SCALE2 - (m_new - lift if biased else m_new))
        shrink = jnp.exp2(m_old - m_new)
        l_s[k, h] = l_s[k, h] * shrink + jnp.sum(p, axis=0, keepdims=True)
        m_s[k, h] = m_new
        return p.astype(BF16), shrink

    def pass_on(s, j):
        landed(zka.at[0, 0:2], 13 + 4 * s + j)
        if s < 3 or j < 2:
            go_right(s + 1, j).start()
        if s < 3 or j >= 2:
            go_left(s + 1, j).start()

    def project(n, k):
        return dot(lows[0:n], uk[k]).astype(BF16), dot_nt(wv_t[k], lows[0:n]).astype(BF16)

    def score(nope, n, k, h):
        key = jnp.concatenate([nope[:, 128 * h : 128 * h + 128], ropes[0:n]], axis=1)
        return dot(key, q_t[k, h])

    def weigh(s_ref, n, k, h, biased):
        p, shrink = softmax(s_ref, n, k, h, biased)
        acc[k, h] = acc[k, h] * shrink + dot(vt[128 * h : 128 * h + 128, 0:n], p)

    def attend(n, stage, biased, passes, finish):
        def step(k, final):
            for at, s, j in passes:
                if final and at == NY - 1:
                    pass_on(s, j)
                elif not final and at < NY - 1:
                    pl.when(k == at)(lambda s=s, j=j: pass_on(s, j))
            sb[0:n] = score(kn[0:n], n, k, 1)
            if not final:
                nope, val = project(n, k + 1)
            weigh(sa, n, k, 0, biased)
            if final:
                finish(k, 0)
            else:
                sa[0:n] = score(nope, n, k + 1, 0)
            weigh(sb, n, k, 1, biased)
            if not final:
                kn[0:n] = nope
                vt[:, 0:n] = val
                finish(k, 0)
            finish(k, 1)

        stage()
        nope, val = project(n, 0)
        kn[0:n] = nope
        vt[:, 0:n] = val
        sa[0:n] = score(nope, n, 0, 0)

        @pl.loop(0, NY - 1)
        def _(k):
            step(k, False)

        step(NY - 1, True)

    def stage_context():
        both = ctx[...].reshape(CTXK, 384)
        lows[0:CTXK] = both[:, :256]
        ropes[0:CTXK] = both[:, 256:]

    def stage_a(at, offset):
        slot = slot_of(offset)
        lows[at : at + BUNDLE] = zka[slot, :, :ROWS_A].reshape(BUNDLE, 256)
        for i in range(NX):
            run = zka[slot, i, ROWS_A:]
            for g in range(4):
                tile = run[:, 128 * (g // 2) : 128 * (g // 2) + 128]
                first = at + ROWS_A * i + 16 * g
                ropes[first : first + 16] = lane_pair(tile) if g % 2 else tile

    def stage_b(at, line):
        lows[at : at + NZ * ROWS_B] = zkb[line, :, :ROWS_B].reshape(NZ * ROWS_B, 256)
        for i in range(NZ):
            tile = zkb[line, i, ROWS_B:, :128]
            first = at + ROWS_B * i
            ropes[first : first + 16] = tile
            ropes[first + 16 : first + 32] = lane_pair(tile)

    def out_copy(k, h, d):
        return remote(ob.at[k, h, yp[d]], rb.at[k, d - 1, h], snd.at[17], rcv.at[34 + k], y=yp[d])

    def stat_copy(k, d):
        return remote(st.at[yp[d], k], rst.at[k, d - 1], snd.at[18], rcv.at[38 + k], y=yp[d])

    def finish(k, h):
        total = l_s[k, h]
        row = m_s[k, h] + jnp.log2(total)
        for j in range(NY):
            st[j, k, h : h + 1] = jnp.concatenate(
                [row[:, ROWS * j : ROWS * j + ROWS], jnp.zeros((1, 32), F32)], axis=1
            )
        ob[k, h] = (acc[k, h] / total).T.astype(BF16).reshape(NY, ROWS, 128)
        for d in range(1, NY):
            if h == 1:
                stat_copy(k, d).start()
            out_copy(k, h, d).start()

    def stage_first():
        stage_b(0, x)
        stage_a(BUNDLE, -1)
        stage_a(2 * BUNDLE, 1)

    def stage_second():
        stage_a(0, -2)
        stage_a(BUNDLE, 2)

    def stage_last():
        for i, offset in enumerate((-3, 3, 4)):
            stage_a(i * BUNDLE, offset)
        for d in range(1, NX):
            stage_b((2 + d) * BUNDLE, xp[NX - d])

    def nothing(*_):
        pass

    landed(zkb.at[0, 0:2], 30)
    along_z(-2, 3, right).start()
    along_z(2, 5, left).start()

    @pl.when(z % 2 == 0)
    def _():
        along_z(-2, 4, zp[2]).start()

    @pl.when(z % 2 == 1)
    def _():
        along_z(2, 4, zp[6]).start()

    landed(zkb.at[0, 0:2], 31)
    for o in (1, 7, 2, 6):
        for d in nearest:
            along_x(o, d).start()
    attend(CTXK, stage_context, True, ((2, 1, 0), (3, 1, 1)), nothing)
    attend(BUNDLE, lambda: stage_a(0, 0), False, ((1, 1, 2), (3, 1, 3)), nothing)
    landed(zkb.at[0, 0:3], 32)
    for o in (3, 5, 4):
        for d in nearest:
            along_x(o, d).start()
    attend(
        3 * BUNDLE, stage_first, False,
        ((0, 2, 0), (1, 2, 1), (1, 2, 2), (2, 2, 3), (2, 3, 0), (3, 3, 1), (3, 3, 2)), nothing,
    )
    attend(2 * BUNDLE, stage_second, False, ((0, 3, 3),), nothing)
    landed(zka.at[0], 29)
    landed(zkb.at[0:3], 33)
    attend(LAST, stage_last, False, (), finish)

    fetches[16].wait()
    fill = jnp.zeros((6, 128), F32)
    for k in range(NY):
        landed(rst.at[k], 38 + k)
        landed(rb.at[k], 34 + k)
        stats = [st[y, k]] + [rst[k, d - 1] for d in range(1, NY)]
        top = jnp.maximum(jnp.maximum(stats[0], stats[1]), jnp.maximum(stats[2], stats[3]))
        raised = [jnp.exp2(v - top) for v in stats]
        whole = raised[0] + raised[1] + raised[2] + raised[3]
        shares = [jnp.concatenate([r / whole, fill], axis=0).T[:ROWS] for r in raised]
        both = []
        for h in range(2):
            pieces = [ob[k, h, y]] + [rb[k, d - 1, h] for d in range(1, NY)]
            both.append(sum(
                p.astype(F32) * share[:, h : h + 1] for p, share in zip(pieces, shares)
            ))
        part = dot(jnp.concatenate(both, axis=1).astype(BF16), ow[256 * k : 256 * k + 256])
        if k == 0:
            mixed[...] = part
        elif k < NY - 1:
            mixed[...] += part
        else:
            out[...] = (
                lat[...].astype(F32) + gate_s[...] * (mixed[...] + part)
            ).astype(BF16)

    for ref, i in (
        (mod_x.at[0:3], 0), (cx.at[0:3], 1), (mod_z.at[0:7], 2), (mod_y.at[0:3], 3),
        (uq.at[0, 0:192], 5), (uk.at[0:3, 0:128], 6), (uv.at[0:3, 0:128], 7),
        (uq.at[0:3, 0:192], 8), (uq.at[0:3, 0:256], 9), (uk.at[0:3, 0:128], 10),
        (uv.at[0:3, 0:128], 11), (qa.at[0:3], 12), (zka.at[0, 0:3], 13), (zka.at[0:7], 14),
        (zkb.at[0, 0:7], 15), (zkb.at[0:3], 16), (ob.at[:, :, 0:3], 17), (st.at[0:3], 18),
    ):
        drain(ref, i)

    @pl.when(mine)
    def _():
        drain(uq.at[0, 0:448], 4)


def rope_constants():
    inverse = (10000.0 ** (-np.arange(16, dtype=np.float64) / 16)).astype(np.float32)

    def spread(count, first):
        angles = (np.arange(count, dtype=np.float32)[:, None] * inverse).astype(np.float64)
        zero = np.zeros((count, 32))
        runs = []
        for f in (np.cos, np.sin):
            pair = np.concatenate([f(angles), f(angles)], axis=1)
            runs += [pair, zero] if first else [zero, pair]
        return np.concatenate(runs, axis=1).astype(np.float32)

    return spread(192, True), spread(GRID_W, False)


def on_device(
    latent_in, condition, context_latent, context_rope, shift_weight, scale_weight, gate_weight,
    norm_gain, down_query, down_latent, down_rope, query_gain, latent_gain, up_query, up_key,
    up_value, context_bias, out_weight,
):
    row_table, col_table = rope_constants()
    vmem = pltpu.VMEM
    dma = pltpu.SemaphoreType.DMA
    return pl.pallas_call(
        kernel,
        name="whole",
        out_shape=jax.ShapeDtypeStruct((ROWS, D), BF16),
        in_specs=[pl.BlockSpec(memory_space=pltpu.HBM)] * 20,
        out_specs=pl.BlockSpec(memory_space=pltpu.VMEM),
        scratch_shapes=[
            vmem((1, 64), BF16),
            vmem((64, 512), BF16), vmem((64, 512), BF16), vmem((64, 512), BF16),
            vmem((1, 2), F32),
            vmem((ROWS, D), BF16),
            vmem((1, D), F32), vmem((1, 512), F32), vmem((1, 256), F32),
            vmem((192, 128), F32), vmem((GRID_W, 128), F32),
            vmem((16, 256), BF16), vmem((16, 64), BF16),
            vmem((D, 512), BF16), vmem((D, 256), BF16), vmem((64, D), BF16),
            vmem((1024, D), BF16),
            vmem((NY, 512, 384), BF16), vmem((NY, 256, 256), BF16), vmem((NY, 256, 256), BF16),
            vmem((NX, 3, 512), F32), vmem((NZ, 3, 512), F32), vmem((NY, 4, 512), F32),
            vmem((16, 384), BF16), vmem((NX, 16, 384), BF16), vmem((8, 16, 384), BF16),
            vmem((ROWS, 512), BF16),
            vmem((1, D), F32), vmem((NY, 128), F32),
            vmem((NY, ROWS, 512), BF16),
            vmem((NZ, NX, PIECE_A, 256), BF16), vmem((NX, NZ, PIECE_B, 256), BF16),
            vmem((NY, 384, 512), BF16), vmem((NY, 256, 256), BF16),
            vmem((NY, 2, 256, QN), BF16),
            vmem((LAST, 256), BF16), vmem((LAST, 128), BF16),
            vmem((LAST, 256), BF16), vmem((256, LAST), BF16),
            vmem((LAST, QN), F32), vmem((LAST, QN), F32),
            vmem((NY, 2, 1, QN), F32), vmem((NY, 2, 1, QN), F32),
            vmem((NY, 2, 128, QN), F32),
            vmem((NY, 2, NY, ROWS, 128), BF16), vmem((NY, NY - 1, 2, ROWS, 128), BF16),
            vmem((NY, NY, 2, 128), F32), vmem((NY, NY - 1, 2, 128), F32),
            vmem((ROWS, D), F32),
            dma((17,)), dma((3,)), dma((19,)), dma((42,)),
        ],
        compiler_params=pltpu.CompilerParams(
            collective_id=0, has_side_effects=True, vmem_limit_bytes=60 * 1024 * 1024
        ),
    )(
        condition.reshape(1, -1), shift_weight, scale_weight, gate_weight,
        context_bias.reshape(1, -1), latent_in, norm_gain.reshape(1, -1),
        query_gain.reshape(1, -1), latent_gain.reshape(1, -1), jnp.asarray(row_table),
        jnp.asarray(col_table), context_latent, context_rope, down_query, down_latent,
        down_rope.T, up_query, up_key, up_value, out_weight,
    )


def solution(mesh):
    split = Mesh(mesh.devices.reshape(NZ, NX, NY, 2), ("z", "x", "y", "c"))
    rows = P(("c", "z", "x", "y"), None)
    held = P(("c", "z", "x"), None)
    weight = P(("z", "x"), "y")
    placed = (
        rows, P(("c", "z", "x")), held, held, weight, weight, weight, P(), P(), P(), P(), P(),
        P(), P(None, "y"), P(None, "y"), P(None, "y"), P("y"), P(),
    )
    return jax.shard_map(
        on_device, mesh=split, in_specs=placed, out_specs=rows, check_vma=False
    )
```

```python
import math

import jax
import jax.numpy as jnp
import numpy as np
from jax import lax
from jax.experimental import pallas as pl
from jax.experimental.pallas import tpu as pltpu
from jax.sharding import Mesh
from jax.sharding import PartitionSpec as P

ROWS = 96
D = 2048
NZ, NX, NY = 8, 4, 4
GRID_W = 64
CTXK = 128
EPS = 1e-06
QN = NY * ROWS
ROWS_A, ROWS_B = 64, 32
PIECE_A, PIECE_B = ROWS_A + 16, ROWS_B + 16
BUNDLE = NX * ROWS_A
LAST = 3 * BUNDLE + (NX - 1) * NZ * ROWS_B
LOG2E = math.log2(math.e)
SCALE2 = LOG2E / math.sqrt(192.0)
MESH = pl.DeviceIdType.MESH
F32 = jnp.float32
BF16 = jnp.bfloat16
NEG = float("-inf")


def dot(a, b):
    return jnp.dot(a, b, preferred_element_type=F32)


def dot_nt(a, b):
    return lax.dot_general(a, b, (((1,), (1,)), ((), ())), preferred_element_type=F32)


def remote(src, dst, send_sem, recv_sem, **where):
    return pltpu.make_async_remote_copy(
        src_ref=src, dst_ref=dst, send_sem=send_sem, recv_sem=recv_sem,
        device_id=where, device_id_type=MESH,
    )


def lane_pair(run):
    return jnp.concatenate([run[:, 64:], run[:, :64]], axis=1)


def piece_order(k):
    return k + (k // 2) * (5 - 2 * k)


def kernel(
    cond_h, sw_h, cw_h, gw_h, bias_h, lat_h, gain_h, qg_h, lg_h, rowt_h, colt_h, ctxl_h, ctxr_h,
    dq_h, dl_h, dr_h, uq_h, uk_h, uv_h, ow_h,
    out,
    cond, sw, cw, gw, bias, lat, gain, qg, lg, rowt, colt, ctxl, ctxr, dq, dl, dr, ow,
    uq, uk, uv, mod_x, mod_z, mod_y, cblk, cx, ctx, qlow, gate_s, bias_s,
    qa, zka, zkb, wq_t, wv_t, q_t, lows, ropes, kn, vt, sa, sb, m_s, l_s, acc, ob, rb, st, rst, mixed,
    in_sem, own_sem, snd, rcv,
):
    z, x, y, c = (lax.axis_index(n) for n in ("z", "x", "y", "c"))
    sp = z * NX + x

    def drain(ref, i):
        remote(ref, ref, snd.at[i], rcv.at[0], c=1 - c).wait_send()

    def landed(ref, i):
        remote(ref, ref, snd.at[0], rcv.at[i], c=1 - c).wait_recv()

    fetches = [
        pltpu.make_async_copy(h, v, in_sem.at[i])
        for i, (h, v) in enumerate((
            (cond_h, cond), (sw_h, sw), (cw_h, cw), (gw_h, gw), (bias_h, bias), (ctxl_h, ctxl),
            (ctxr_h, ctxr), (lat_h, lat), (gain_h, gain), (qg_h, qg), (lg_h, lg),
            (rowt_h, rowt), (colt_h, colt), (dq_h, dq), (dl_h, dl), (dr_h, dr), (ow_h, ow),
        ))
    ]
    owns = [
        pltpu.make_async_copy(h, v.at[y], own_sem.at[i])
        for i, (h, v) in enumerate(((uq_h, uq), (uk_h, uk), (uv_h, uv)))
    ]
    for copy in fetches[:7] + owns:
        copy.start()
    xp = [lax.rem(x + d, NX) for d in range(NX)]
    yp = [lax.rem(y + d, NY) for d in range(NY)]
    zp = [lax.rem(z + d, NZ) for d in range(NZ)]
    right, left = zp[1], zp[NZ - 1]
    farthest = (2, 1, 3)
    peers = (
        [{"x": xp[d]} for d in range(1, NX)]
        + [{"y": yp[d]} for d in range(1, NY)]
        + [{"z": zp[d]} for d in range(1, NZ)]
        + [{"c": 1 - c}]
    )
    barrier = pltpu.get_barrier_semaphore()
    for where in peers:
        pl.semaphore_signal(barrier, inc=1, device_id=where, device_id_type=MESH)

    for copy in fetches[:7]:
        copy.wait()
    v = cond[...].astype(F32)
    activated = (v / (1.0 + jnp.exp(-v))).astype(BF16)
    mod_x[x] = jnp.concatenate([dot(activated, w[...]) for w in (sw, cw, gw)], axis=0)
    pl.semaphore_wait(barrier, len(peers))
    xcopies = [
        remote(mod_x.at[x], mod_x.at[x], snd.at[0], rcv.at[0], x=xp[d]) for d in farthest
    ]
    for copy in xcopies:
        copy.start()
    for copy in fetches[7:]:
        copy.start()
    for copy in owns:
        copy.wait()
    cblk[...] = jnp.concatenate([ctxl[...], ctxr[...], jnp.zeros((16, 64), BF16)], axis=1)
    cx[x] = cblk[...]
    ccopies = [remote(cblk, cx.at[x], snd.at[1], rcv.at[1], x=xp[d]) for d in farthest]
    for copy in ccopies:
        copy.start()

    def half(ref, slot):
        rows = ref.shape[1] // 2
        return ref.at[slot, pl.ds(pl.multiple_of(c * rows, rows), rows)]

    def eighth(slot):
        return uq.at[slot, pl.ds(pl.multiple_of(c * 256 + x * 64, 64), 64)]

    def over_y(d, i):
        return remote(half(ups[i], y), half(ups[i], y), snd.at[5 + i], rcv.at[6 + i], y=yp[d])

    def eighth_over_y(d):
        return remote(eighth(y), eighth(y), snd.at[5], rcv.at[6], y=yp[d])

    def eighth_over_x(d, e):
        slot = yp[NY - d]
        return remote(eighth(slot), eighth(slot), snd.at[8], rcv.at[9], x=xp[e])

    def across(d, i):
        slot = yp[NY - d]
        return remote(half(ups[i], slot), half(ups[i], slot), snd.at[9 + i], rcv.at[10 + i], c=1 - c)

    ups = (uq, uk, uv)
    for d in farthest:
        eighth_over_y(d).start()
    for d in farthest:
        over_y(d, 1).start()

    landed(mod_x.at[0:3], 0)
    mod_z[z] = mod_x[0] + mod_x[1] + mod_x[2] + mod_x[3]
    zcopies = [
        remote(mod_z.at[z], mod_z.at[z], snd.at[2], rcv.at[2], z=zp[d])
        for d in (4, 3, 5, 2, 6, 1, 7)
    ]
    for copy in zcopies:
        copy.start()
    for copy in fetches[7:13]:
        copy.wait()
    lat32 = lat[...].astype(F32)
    inv = lax.rsqrt(jnp.mean(lat32 * lat32, axis=-1, keepdims=True) + EPS)
    scaled = lat32 * inv * gain[...]
    line = [rowt[pl.ds(sp * 6 + i, 1), :] + colt[...] for i in range(6)]
    line_t = jnp.concatenate(line, axis=0).T
    own_table = []
    for t in range(3):
        g = y * 3 + t
        own_table.append(
            rowt[pl.ds(sp * 6 + g // 2, 1), :]
            + colt[pl.ds(pl.multiple_of((g % 2) * 32, 32), 32), :]
        )
    own_table = jnp.concatenate(own_table, axis=0)
    wq_t[y] = uq[y].T
    wv_t[y] = uv[y].T
    m_s[...] = jnp.full(m_s.shape, NEG, F32)
    l_s[...] = jnp.zeros(l_s.shape, F32)
    acc[...] = jnp.zeros(acc.shape, F32)
    landed(cx.at[0:3], 1)
    mine = z // 2 == y
    zc = [
        remote(
            cx, ctx.at[pl.ds(pl.multiple_of((z % 2) * NX, NX), NX)], snd.at[4],
            rcv.at[4 + z % 2], z=zp[d],
        )
        for d in range(1, NZ)
    ]

    @pl.when(mine)
    def _():
        ctx[pl.ds((z % 2) * NX, NX)] = cx[...]
        for copy in zc:
            copy.start()

    landed(uq.at[0, 0:192], 6)
    for d in farthest:
        for e in farthest:
            eighth_over_x(d, e).start()

    landed(mod_z.at[0:7], 2)
    total = mod_z[0]
    for k in range(1, NZ):
        total = total + mod_z[k]
    bias_row = jnp.concatenate([bias[...], jnp.zeros((1, 510), F32)], axis=1)
    mod_y[y] = jnp.concatenate([total, bias_row], axis=0)
    ycopies = [
        remote(mod_y.at[y], mod_y.at[y], snd.at[3], rcv.at[3], y=yp[d]) for d in farthest
    ]
    for copy in ycopies:
        copy.start()
    for d in farthest:
        over_y(d, 2).start()
    landed(uk.at[0:3, 0:128], 7)
    for d in farthest:
        across(d, 1).start()

    landed(mod_y.at[0:3], 3)
    landed(uq.at[0:3, 0:192], 9)
    for d in farthest:
        across(d, 0).start()
    shift = jnp.concatenate([mod_y[k, 0:1] for k in range(NY)], axis=1)
    scale = jnp.concatenate([mod_y[k, 1:2] for k in range(NY)], axis=1)
    gate_s[...] = jnp.concatenate([mod_y[k, 2:3] for k in range(NY)], axis=1)
    bias_s[...] = jnp.concatenate([mod_y[k, 3:4, 0:128] for k in range(NY)], axis=0)
    normed = (scaled * (1.0 + scale) + shift).astype(BF16)
    for copy in fetches[13:16]:
        copy.wait()

    def rms(a, g):
        return a * lax.rsqrt(jnp.mean(a * a, axis=-1, keepdims=True) + EPS) * g

    qlow[...] = rms(dot(normed, dq[...]), qg[...]).astype(BF16)
    qcopies = [remote(qlow, qa.at[y], snd.at[12], rcv.at[13], y=yp[d]) for d in farthest]
    for copy in qcopies:
        copy.start()
    low = rms(dot(normed, dl[...]), lg[...]).astype(BF16)
    u = dot_nt(normed, dr[...])
    turned = jnp.concatenate([-u[:, 16:32], u[:, 0:16], -u[:, 48:64], u[:, 32:48]], axis=1)
    rope = u * own_table[:, :64] + turned * own_table[:, 64:]
    runs = [rope[16 * g : 16 * g + 16] for g in range(6)]
    zka[z, x] = jnp.concatenate(
        [low[:ROWS_A], jnp.concatenate(runs[:4], axis=1).astype(BF16)], axis=0
    )
    zkb[x, z] = jnp.concatenate(
        [
            low[ROWS_A:],
            jnp.concatenate(runs[4:] + [jnp.zeros((16, 128), F32)], axis=1).astype(BF16),
        ],
        axis=0,
    )

    def slot_of(offset):
        return lax.rem(z + offset + NZ, NZ)

    def piece(offset, j):
        return zka.at[slot_of(offset), lax.rem(x - piece_order(j) + NX, NX)]

    def turn(s, j):
        return rcv.at[13 + 4 * s + j]

    def go_right(s, j):
        return remote(piece(1 - s, j), piece(1 - s, j), snd.at[14], turn(s, j), z=right)

    def go_left(s, j):
        return remote(piece(s - 1, j), piece(s - 1, j), snd.at[14], turn(s, j), z=left)

    def two_right(j):
        return remote(piece(-2, j), piece(-2, j), snd.at[14], rcv.at[29], z=zp[2])

    def two_left(j):
        return remote(piece(2, j), piece(2, j), snd.at[14], rcv.at[29], z=zp[NZ - 2])

    def pass_on(s, j):
        landed(zka.at[0, 0:2], 13 + 4 * s + j)
        go_right(s + 1, j).start()
        go_left(s + 1, j).start()
        if s == 2:
            (two_right if j < 2 else two_left)(j).start()

    kcopies = [
        remote(zka.at[z, x], zka.at[z, x], snd.at[13], rcv.at[13 + d], x=xp[d]) for d in range(1, NX)
    ]
    def along_z(origin, d, to):
        held = zkb.at[x, slot_of(origin)]
        group = 30 if d in (2, 6) else 31 if d in (1, 7) else 32
        return remote(held, held, snd.at[15], rcv.at[group], z=to)

    def along_x(o, d):
        held = zkb.at[x, slot_of(-o)]
        return remote(held, held, snd.at[16], rcv.at[33], x=xp[d])

    for d in farthest:
        kcopies[d - 1].start()
    go_right(1, 0).start()
    go_left(1, 0).start()
    for d in (2, 6, 1, 7):
        along_z(0, d, zp[d]).start()
    for d in farthest:
        along_x(0, d).start()
    qa[y] = qlow[...]

    landed(uv.at[0:3, 0:128], 8)
    for d in farthest:
        across(d, 2).start()
    landed(uq.at[0:3, 0:256], 10)
    for d in farthest:
        slot = yp[NY - d]
        wq_t[slot] = uq[slot].T
    pass_on(1, 0)
    for j, d in ((1, 1), (2, 3), (3, 2)):
        kcopies[d - 1].wait_recv()
        go_right(1, j).start()
        go_left(1, j).start()
    landed(uk.at[0:3, 0:128], 11)
    landed(uv.at[0:3, 0:128], 12)
    for d in farthest:
        slot = yp[NY - d]
        wv_t[slot] = uv[slot].T
    for k in range(2):
        @pl.when(z != 2 * y + k)
        def _():
            landed(ctx.at[pl.ds(k * NX, NX)], 4 + k)

    landed(qa.at[0:3], 13)

    for k in range(NY):
        qt = dot_nt(wq_t[k], qa[...].reshape(QN, 512))
        for h in range(2):
            b = 192 * h
            u = qt[b + 128 : b + 192]
            turned = jnp.concatenate([-u[16:32], u[0:16], -u[48:64], u[32:48]], axis=0)
            rope = u * line_t[:64] + turned * line_t[64:]
            q_t[k, h] = jnp.concatenate(
                [qt[b : b + 128], rope, jnp.zeros((64, QN), F32)], axis=0
            ).astype(BF16)

    def softmax(s_ref, n, k, h, biased):
        parts = [(biased, n, 0.0)]
        if biased:
            parts = [(0, biased, bias_s[pl.ds(k, 1), h : h + 1] * LOG2E)] + parts
        m_old = m_new = m_s[k, h]
        for a, b, lift in parts:
            top = jnp.max(s_ref[a:b], axis=0, keepdims=True) * SCALE2
            m_new = jnp.maximum(m_new, top + lift)
        p = jnp.concatenate(
            [jnp.exp2(s_ref[a:b] * SCALE2 - (m_new - lift)) for a, b, lift in parts], axis=0
        )
        shrink = jnp.exp2(m_old - m_new)
        l_s[k, h] = l_s[k, h] * shrink + jnp.sum(p, axis=0, keepdims=True)
        m_s[k, h] = m_new
        return p.astype(BF16), shrink

    def project(n, k):
        return dot(lows[0:n], uk[k]).astype(BF16), dot_nt(wv_t[k], lows[0:n]).astype(BF16)

    def score(nope, n, k, h):
        key = jnp.concatenate([nope[:, 128 * h : 128 * h + 128], ropes[0:n]], axis=1)
        return dot(key, q_t[k, h])

    def weigh(s_ref, n, k, h, biased):
        p, shrink = softmax(s_ref, n, k, h, biased)
        acc[k, h] = acc[k, h] * shrink + dot(vt[128 * h : 128 * h + 128, 0:n], p)

    def attend(n, stage, biased, passes, finish):
        def step(k, final):
            for at, s, j in passes:
                if final and at == NY - 1:
                    pass_on(s, j)
                elif not final and at < NY - 1:
                    pl.when(k == at)(lambda s=s, j=j: pass_on(s, j))
            sb[0:n] = score(kn[0:n], n, k, 1)
            if not final:
                nope, val = project(n, k + 1)
            weigh(sa, n, k, 0, biased)
            if final:
                finish(k, 0)
            else:
                sa[0:n] = score(nope, n, k + 1, 0)
            weigh(sb, n, k, 1, biased)
            if not final:
                kn[0:n] = nope
                vt[:, 0:n] = val
                finish(k, 0)
            finish(k, 1)

        stage()
        nope, val = project(n, 0)
        kn[0:n] = nope
        vt[:, 0:n] = val
        sa[0:n] = score(nope, n, 0, 0)

        @pl.loop(0, NY - 1)
        def _(k):
            step(k, False)

        step(NY - 1, True)

    def stage_a(at, offset):
        slot = slot_of(offset)
        lows[at : at + BUNDLE] = zka[slot, :, :ROWS_A].reshape(BUNDLE, 256)
        for i in range(NX):
            run = zka[slot, i, ROWS_A:]
            for g in range(4):
                tile = run[:, 128 * (g // 2) : 128 * (g // 2) + 128]
                first = at + ROWS_A * i + 16 * g
                ropes[first : first + 16] = lane_pair(tile) if g % 2 else tile

    def stage_b(at, line):
        lows[at : at + NZ * ROWS_B] = zkb[line, :, :ROWS_B].reshape(NZ * ROWS_B, 256)
        for i in range(NZ):
            tile = zkb[line, i, ROWS_B:, :128]
            first = at + ROWS_B * i
            ropes[first : first + 16] = tile
            ropes[first + 16 : first + 32] = lane_pair(tile)

    def out_copy(k, h, d):
        return remote(ob.at[k, h, yp[d]], rb.at[k, d - 1, h], snd.at[17], rcv.at[34 + k], y=yp[d])

    def stat_copy(k, d):
        return remote(st.at[yp[d], k], rst.at[k, d - 1], snd.at[18], rcv.at[38 + k], y=yp[d])

    def finish(k, h):
        total = l_s[k, h]
        row = m_s[k, h] + jnp.log2(total)
        for j in range(NY):
            st[j, k, h : h + 1] = jnp.concatenate(
                [row[:, ROWS * j : ROWS * j + ROWS], jnp.zeros((1, 32), F32)], axis=1
            )
        ob[k, h] = (acc[k, h] / total).T.astype(BF16).reshape(NY, ROWS, 128)
        for d in farthest:
            if h == 1:
                stat_copy(k, d).start()
            out_copy(k, h, d).start()

    def stage_own():
        both = ctx[...].reshape(CTXK, 384)
        lows[0:CTXK] = both[:, :256]
        ropes[0:CTXK] = both[:, 256:]
        stage_a(CTXK, 0)

    def stage_first():
        stage_b(0, x)
        stage_a(BUNDLE, -1)
        stage_a(2 * BUNDLE, 1)

    def stage_second():
        stage_a(0, -2)
        stage_a(BUNDLE, 2)

    def stage_last():
        for i, offset in enumerate((-3, 3, 4)):
            stage_a(i * BUNDLE, offset)
        for d in range(1, NX):
            stage_b((2 + d) * BUNDLE, xp[NX - d])

    def nothing(*_):
        pass

    landed(zkb.at[0, 0:2], 30)
    along_z(-2, 3, right).start()
    along_z(2, 5, left).start()

    @pl.when(z % 2 == 0)
    def _():
        along_z(-2, 4, zp[2]).start()

    @pl.when(z % 2 == 1)
    def _():
        along_z(2, 4, zp[6]).start()

    landed(zkb.at[0, 0:2], 31)
    for o in (1, 7, 2, 6):
        for d in farthest:
            along_x(o, d).start()
    attend(CTXK + BUNDLE, stage_own, CTXK, ((1, 2, 0), (3, 1, 1)), nothing)
    pass_on(1, 2)
    pass_on(1, 3)
    landed(zkb.at[0, 0:3], 32)
    for o in (3, 5, 4):
        for d in farthest:
            along_x(o, d).start()
    attend(
        3 * BUNDLE, stage_first, 0,
        ((1, 2, 1), (2, 2, 2), (3, 2, 3)), nothing,
    )
    attend(2 * BUNDLE, stage_second, 0, (), nothing)
    for j in range(NX):
        landed(zka.at[0, 0:2], 25 + j)
    landed(zka.at[0], 29)
    landed(zkb.at[0:3], 33)
    attend(LAST, stage_last, 0, (), finish)

    fetches[16].wait()
    fill = jnp.zeros((6, 128), F32)
    for k in range(NY):
        landed(rst.at[k], 38 + k)
        landed(rb.at[k], 34 + k)
        stats = [st[y, k]] + [rst[k, d - 1] for d in range(1, NY)]
        top = jnp.maximum(jnp.maximum(stats[0], stats[1]), jnp.maximum(stats[2], stats[3]))
        raised = [jnp.exp2(v - top) for v in stats]
        whole = raised[0] + raised[1] + raised[2] + raised[3]
        shares = [jnp.concatenate([r / whole, fill], axis=0).T[:ROWS] for r in raised]
        both = []
        for h in range(2):
            pieces = [ob[k, h, y]] + [rb[k, d - 1, h] for d in range(1, NY)]
            both.append(sum(
                p.astype(F32) * share[:, h : h + 1] for p, share in zip(pieces, shares)
            ))
        part = dot(jnp.concatenate(both, axis=1).astype(BF16), ow[256 * k : 256 * k + 256])
        if k == 0:
            mixed[...] = part
        elif k < NY - 1:
            mixed[...] += part
        else:
            out[...] = (
                lat[...].astype(F32) + gate_s[...] * (mixed[...] + part)
            ).astype(BF16)

    for ref, i in (
        (mod_x.at[0:3], 0), (cx.at[0:3], 1), (mod_z.at[0:7], 2), (mod_y.at[0:3], 3),
        (uq.at[0, 0:192], 5), (uk.at[0:3, 0:128], 6), (uv.at[0:3, 0:128], 7),
        (uq.at[0:3, 0:192], 8), (uq.at[0:3, 0:256], 9), (uk.at[0:3, 0:128], 10),
        (uv.at[0:3, 0:128], 11), (qa.at[0:3], 12), (zka.at[0, 0:3], 13), (zka.at[0:7], 14),
        (zkb.at[0, 0:7], 15), (zkb.at[0:3], 16), (ob.at[:, :, 0:3], 17), (st.at[0:3], 18),
    ):
        drain(ref, i)

    @pl.when(mine)
    def _():
        drain(uq.at[0, 0:448], 4)


def rope_constants():
    inverse = (10000.0 ** (-np.arange(16, dtype=np.float64) / 16)).astype(np.float32)

    def spread(count, first):
        angles = (np.arange(count, dtype=np.float32)[:, None] * inverse).astype(np.float64)
        zero = np.zeros((count, 32))
        runs = []
        for f in (np.cos, np.sin):
            pair = np.concatenate([f(angles), f(angles)], axis=1)
            runs += [pair, zero] if first else [zero, pair]
        return np.concatenate(runs, axis=1).astype(np.float32)

    return spread(192, True), spread(GRID_W, False)


def on_device(
    latent_in, condition, context_latent, context_rope, shift_weight, scale_weight, gate_weight,
    norm_gain, down_query, down_latent, down_rope, query_gain, latent_gain, up_query, up_key,
    up_value, context_bias, out_weight,
):
    row_table, col_table = rope_constants()
    vmem = pltpu.VMEM
    dma = pltpu.SemaphoreType.DMA
    hold = lambda a: pltpu.with_memory_space_constraint(a, pltpu.HBM)
    return pl.pallas_call(
        kernel,
        name="whole",
        out_shape=jax.ShapeDtypeStruct((ROWS, D), BF16),
        in_specs=[pl.BlockSpec(memory_space=pltpu.HBM)] * 20,
        out_specs=pl.BlockSpec(memory_space=pltpu.VMEM),
        scratch_shapes=[
            vmem((1, 64), BF16),
            vmem((64, 512), BF16), vmem((64, 512), BF16), vmem((64, 512), BF16),
            vmem((1, 2), F32),
            vmem((ROWS, D), BF16),
            vmem((1, D), F32), vmem((1, 512), F32), vmem((1, 256), F32),
            vmem((192, 128), F32), vmem((GRID_W, 128), F32),
            vmem((16, 256), BF16), vmem((16, 64), BF16),
            vmem((D, 512), BF16), vmem((D, 256), BF16), vmem((64, D), BF16),
            vmem((1024, D), BF16),
            vmem((NY, 512, 384), BF16), vmem((NY, 256, 256), BF16), vmem((NY, 256, 256), BF16),
            vmem((NX, 3, 512), F32), vmem((NZ, 3, 512), F32), vmem((NY, 4, 512), F32),
            vmem((16, 384), BF16), vmem((NX, 16, 384), BF16), vmem((8, 16, 384), BF16),
            vmem((ROWS, 512), BF16),
            vmem((1, D), F32), vmem((NY, 128), F32),
            vmem((NY, ROWS, 512), BF16),
            vmem((NZ, NX, PIECE_A, 256), BF16), vmem((NX, NZ, PIECE_B, 256), BF16),
            vmem((NY, 384, 512), BF16), vmem((NY, 256, 256), BF16),
            vmem((NY, 2, 256, QN), BF16),
            vmem((LAST, 256), BF16), vmem((LAST, 128), BF16),
            vmem((LAST, 256), BF16), vmem((256, LAST), BF16),
            vmem((LAST, QN), F32), vmem((LAST, QN), F32),
            vmem((NY, 2, 1, QN), F32), vmem((NY, 2, 1, QN), F32),
            vmem((NY, 2, 128, QN), F32),
            vmem((NY, 2, NY, ROWS, 128), BF16), vmem((NY, NY - 1, 2, ROWS, 128), BF16),
            vmem((NY, NY, 2, 128), F32), vmem((NY, NY - 1, 2, 128), F32),
            vmem((ROWS, D), F32),
            dma((17,)), dma((3,)), dma((19,)), dma((42,)),
        ],
        compiler_params=pltpu.CompilerParams(
            collective_id=0, has_side_effects=True, vmem_limit_bytes=40 * 1024 * 1024
        ),
    )(*(hold(a) for a in (
        condition.reshape(1, -1), shift_weight, scale_weight, gate_weight,
        context_bias.reshape(1, -1), latent_in, norm_gain.reshape(1, -1),
        query_gain.reshape(1, -1), latent_gain.reshape(1, -1), jnp.asarray(row_table),
        jnp.asarray(col_table), context_latent, context_rope, down_query, down_latent,
        down_rope.T, up_query, up_key, up_value, out_weight,
    )))


def solution(mesh):
    split = Mesh(mesh.devices.reshape(NZ, NX, NY, 2), ("z", "x", "y", "c"))
    rows = P(("c", "z", "x", "y"), None)
    held = P(("c", "z", "x"), None)
    weight = P(("z", "x"), "y")
    placed = (
        rows, P(("c", "z", "x")), held, held, weight, weight, weight, P(), P(), P(), P(), P(),
        P(), P(None, "y"), P(None, "y"), P(None, "y"), P("y"), P(),
    )
    return jax.shard_map(
        on_device, mesh=split, in_specs=placed, out_specs=rows, check_vma=False
    )
```

```python
import math

import jax
import jax.numpy as jnp
import numpy as np
from jax import lax
from jax.experimental import pallas as pl
from jax.experimental.pallas import tpu as pltpu
from jax.sharding import Mesh
from jax.sharding import PartitionSpec as P

ROWS = 96
D = 2048
NZ, NX, NY = 8, 4, 4
GRID_W = 64
CTXK = 128
EPS = 1e-06
QN = NY * ROWS
ROWS_A, ROWS_B = 64, 32
PIECE_A, PIECE_B = ROWS_A + 16, ROWS_B + 16
BUNDLE = NX * ROWS_A
LAST = 3 * BUNDLE + (NX - 2) * NZ * ROWS_B
LOG2E = math.log2(math.e)
SCALE2 = LOG2E / math.sqrt(192.0)
MESH = pl.DeviceIdType.MESH
F32 = jnp.float32
BF16 = jnp.bfloat16
NEG = float("-inf")


def dot(a, b):
    return jnp.dot(a, b, preferred_element_type=F32)


def dot_nt(a, b):
    return lax.dot_general(a, b, (((1,), (1,)), ((), ())), preferred_element_type=F32)


def remote(src, dst, send_sem, recv_sem, **where):
    return pltpu.make_async_remote_copy(
        src_ref=src, dst_ref=dst, send_sem=send_sem, recv_sem=recv_sem,
        device_id=where, device_id_type=MESH,
    )


def lane_pair(run):
    return jnp.concatenate([run[:, 64:], run[:, :64]], axis=1)


def piece_order(k):
    return k + (k // 2) * (5 - 2 * k)


def kernel(
    cond_h, sw_h, cw_h, gw_h, bias_h, lat_h, gain_h, qg_h, lg_h, rowt_h, colt_h, ctxl_h, ctxr_h,
    dq_h, dl_h, dr_h, uq_h, uk_h, uv_h, ow_h,
    out,
    cond, sw, cw, gw, bias, lat, gain, qg, lg, rowt, colt, ctxl, ctxr, dq, dl, dr, ow,
    uq, uk, uv, mod_x, mod_z, mod_y, cblk, cx, ctx, qlow, gate_s, bias_s,
    qa, zka, zkb, wq_t, wv_t, q_t, lows, ropes, kn, vt, sa, sb, m_s, l_s, acc, ob, rb, st, rst, mixed,
    in_sem, own_sem, snd, rcv,
):
    z, x, y, c = (lax.axis_index(n) for n in ("z", "x", "y", "c"))
    sp = z * NX + x

    def drain(ref, i):
        remote(ref, ref, snd.at[i], rcv.at[0], c=1 - c).wait_send()

    def landed(ref, i):
        remote(ref, ref, snd.at[0], rcv.at[i], c=1 - c).wait_recv()

    fetches = [
        pltpu.make_async_copy(h, v, in_sem.at[i])
        for i, (h, v) in enumerate((
            (cond_h, cond), (sw_h, sw), (cw_h, cw), (gw_h, gw), (bias_h, bias), (ctxl_h, ctxl),
            (ctxr_h, ctxr), (lat_h, lat), (gain_h, gain), (qg_h, qg), (lg_h, lg),
            (rowt_h, rowt), (colt_h, colt), (dq_h, dq), (dl_h, dl), (dr_h, dr), (ow_h, ow),
        ))
    ]
    owns = [
        pltpu.make_async_copy(h, v.at[y], own_sem.at[i])
        for i, (h, v) in enumerate(((uq_h, uq), (uk_h, uk), (uv_h, uv)))
    ]
    for copy in fetches[:7] + owns:
        copy.start()
    xp = [lax.rem(x + d, NX) for d in range(NX)]
    yp = [lax.rem(y + d, NY) for d in range(NY)]
    zp = [lax.rem(z + d, NZ) for d in range(NZ)]
    right, left = zp[1], zp[NZ - 1]
    farthest = (2, 1, 3)
    peers = (
        [{"x": xp[d]} for d in range(1, NX)]
        + [{"y": yp[d]} for d in range(1, NY)]
        + [{"z": zp[d]} for d in range(1, NZ)]
        + [{"c": 1 - c}]
    )
    barrier = pltpu.get_barrier_semaphore()
    for where in peers:
        pl.semaphore_signal(barrier, inc=1, device_id=where, device_id_type=MESH)

    for copy in fetches[:7]:
        copy.wait()
    v = cond[...].astype(F32)
    activated = (v / (1.0 + jnp.exp(-v))).astype(BF16)
    mod_x[x] = jnp.concatenate([dot(activated, w[...]) for w in (sw, cw, gw)], axis=0)
    pl.semaphore_wait(barrier, len(peers))
    xcopies = [
        remote(mod_x.at[x], mod_x.at[x], snd.at[0], rcv.at[0], x=xp[d]) for d in farthest
    ]
    for copy in xcopies:
        copy.start()
    for copy in fetches[7:]:
        copy.start()
    for copy in owns:
        copy.wait()
    cblk[...] = jnp.concatenate([ctxl[...], ctxr[...], jnp.zeros((16, 64), BF16)], axis=1)
    cx[x] = cblk[...]
    ccopies = [remote(cblk, cx.at[x], snd.at[1], rcv.at[1], x=xp[d]) for d in farthest]
    for copy in ccopies:
        copy.start()

    def half(ref, slot):
        rows = ref.shape[1] // 2
        return ref.at[slot, pl.ds(pl.multiple_of(c * rows, rows), rows)]

    def eighth(slot):
        return uq.at[slot, pl.ds(pl.multiple_of(c * 256 + x * 64, 64), 64)]

    def over_y(d, i):
        return remote(half(ups[i], y), half(ups[i], y), snd.at[5 + i], rcv.at[6 + i], y=yp[d])

    def eighth_over_y(d):
        return remote(eighth(y), eighth(y), snd.at[5], rcv.at[6], y=yp[d])

    def eighth_over_x(d, e):
        slot = yp[NY - d]
        return remote(eighth(slot), eighth(slot), snd.at[8], rcv.at[9], x=xp[e])

    def across(d, i):
        slot = yp[NY - d]
        return remote(half(ups[i], slot), half(ups[i], slot), snd.at[9 + i], rcv.at[10 + i], c=1 - c)

    ups = (uq, uk, uv)
    for d in farthest:
        eighth_over_y(d).start()
    for d in farthest:
        over_y(d, 1).start()

    landed(mod_x.at[0:3], 0)
    mod_z[z] = mod_x[0] + mod_x[1] + mod_x[2] + mod_x[3]
    zcopies = [
        remote(mod_z.at[z], mod_z.at[z], snd.at[2], rcv.at[2], z=zp[d])
        for d in (4, 3, 5, 2, 6, 1, 7)
    ]
    for copy in zcopies:
        copy.start()
    for copy in fetches[7:13]:
        copy.wait()
    lat32 = lat[...].astype(F32)
    inv = lax.rsqrt(jnp.mean(lat32 * lat32, axis=-1, keepdims=True) + EPS)
    scaled = lat32 * inv * gain[...]
    line = [rowt[pl.ds(sp * 6 + i, 1), :] + colt[...] for i in range(6)]
    line_t = jnp.concatenate(line, axis=0).T
    own_table = []
    for t in range(3):
        g = y * 3 + t
        own_table.append(
            rowt[pl.ds(sp * 6 + g // 2, 1), :]
            + colt[pl.ds(pl.multiple_of((g % 2) * 32, 32), 32), :]
        )
    own_table = jnp.concatenate(own_table, axis=0)
    wq_t[y] = uq[y].T
    wv_t[y] = uv[y].T
    m_s[...] = jnp.full(m_s.shape, NEG, F32)
    l_s[...] = jnp.zeros(l_s.shape, F32)
    acc[...] = jnp.zeros(acc.shape, F32)
    landed(cx.at[0:3], 1)
    mine = z // 2 == y
    zc = [
        remote(
            cx, ctx.at[pl.ds(pl.multiple_of((z % 2) * NX, NX), NX)], snd.at[4],
            rcv.at[4 + z % 2], z=zp[d],
        )
        for d in range(1, NZ)
    ]

    @pl.when(mine)
    def _():
        ctx[pl.ds((z % 2) * NX, NX)] = cx[...]
        for copy in zc:
            copy.start()

    landed(uq.at[0, 0:192], 6)
    for d in farthest:
        for e in farthest:
            eighth_over_x(d, e).start()

    landed(mod_z.at[0:7], 2)
    total = mod_z[0]
    for k in range(1, NZ):
        total = total + mod_z[k]
    bias_row = jnp.concatenate([bias[...], jnp.zeros((1, 510), F32)], axis=1)
    mod_y[y] = jnp.concatenate([total, bias_row], axis=0)
    ycopies = [
        remote(mod_y.at[y], mod_y.at[y], snd.at[3], rcv.at[3], y=yp[d]) for d in farthest
    ]
    for copy in ycopies:
        copy.start()
    for d in farthest:
        over_y(d, 2).start()
    landed(uk.at[0:3, 0:128], 7)
    for d in farthest:
        across(d, 1).start()

    landed(mod_y.at[0:3], 3)
    landed(uq.at[0:3, 0:192], 9)
    for d in farthest:
        across(d, 0).start()
    shift = jnp.concatenate([mod_y[k, 0:1] for k in range(NY)], axis=1)
    scale = jnp.concatenate([mod_y[k, 1:2] for k in range(NY)], axis=1)
    gate_s[...] = jnp.concatenate([mod_y[k, 2:3] for k in range(NY)], axis=1)
    bias_s[...] = jnp.concatenate([mod_y[k, 3:4, 0:128] for k in range(NY)], axis=0)
    normed = (scaled * (1.0 + scale) + shift).astype(BF16)
    for copy in fetches[13:16]:
        copy.wait()

    def rms(a, g):
        return a * lax.rsqrt(jnp.mean(a * a, axis=-1, keepdims=True) + EPS) * g

    qlow[...] = rms(dot(normed, dq[...]), qg[...]).astype(BF16)
    qcopies = [remote(qlow, qa.at[y], snd.at[12], rcv.at[13], y=yp[d]) for d in farthest]
    for copy in qcopies:
        copy.start()
    low = rms(dot(normed, dl[...]), lg[...]).astype(BF16)
    u = dot_nt(normed, dr[...])
    turned = jnp.concatenate([-u[:, 16:32], u[:, 0:16], -u[:, 48:64], u[:, 32:48]], axis=1)
    rope = u * own_table[:, :64] + turned * own_table[:, 64:]
    runs = [rope[16 * g : 16 * g + 16] for g in range(6)]
    zka[z, x] = jnp.concatenate(
        [low[:ROWS_A], jnp.concatenate(runs[:4], axis=1).astype(BF16)], axis=0
    )
    zkb[x, z] = jnp.concatenate(
        [
            low[ROWS_A:],
            jnp.concatenate(runs[4:] + [jnp.zeros((16, 128), F32)], axis=1).astype(BF16),
        ],
        axis=0,
    )

    def slot_of(offset):
        return lax.rem(z + offset + NZ, NZ)

    def piece(offset, j):
        return zka.at[slot_of(offset), lax.rem(x - piece_order(j) + NX, NX)]

    def turn(s, j):
        return rcv.at[13 + 4 * s + j]

    def go_right(s, j):
        return remote(piece(1 - s, j), piece(1 - s, j), snd.at[14], turn(s, j), z=right)

    def go_left(s, j):
        return remote(piece(s - 1, j), piece(s - 1, j), snd.at[14], turn(s, j), z=left)

    def two_right(j):
        return remote(piece(-2, j), piece(-2, j), snd.at[14], rcv.at[29], z=zp[2])

    def two_left(j):
        return remote(piece(2, j), piece(2, j), snd.at[14], rcv.at[29], z=zp[NZ - 2])

    def pass_on(s, j):
        landed(zka.at[0, 0:2], 13 + 4 * s + j)
        go_right(s + 1, j).start()
        go_left(s + 1, j).start()
        if s == 2:
            (two_right if j < 2 else two_left)(j).start()

    kcopies = [
        remote(zka.at[z, x], zka.at[z, x], snd.at[13], rcv.at[13 + d], x=xp[d]) for d in range(1, NX)
    ]
    def along_z(origin, d, to):
        held = zkb.at[x, slot_of(origin)]
        group = 30 if d in (2, 6) else 31 if d in (1, 7) else 32
        return remote(held, held, snd.at[15], rcv.at[group], z=to)

    def along_x(o, d):
        held = zkb.at[x, slot_of(-o)]
        return remote(held, held, snd.at[16], rcv.at[42 if d == 1 else 33], x=xp[d])

    for d in farthest:
        kcopies[d - 1].start()
    go_right(1, 0).start()
    go_left(1, 0).start()
    for d in (2, 6, 1, 7):
        along_z(0, d, zp[d]).start()
    for d in farthest:
        along_x(0, d).start()
    qa[y] = qlow[...]

    landed(uv.at[0:3, 0:128], 8)
    for d in farthest:
        across(d, 2).start()
    landed(uq.at[0:3, 0:256], 10)
    for d in farthest:
        slot = yp[NY - d]
        wq_t[slot] = uq[slot].T
    pass_on(1, 0)
    for j, d in ((1, 1), (2, 3), (3, 2)):
        kcopies[d - 1].wait_recv()
        go_right(1, j).start()
        go_left(1, j).start()
    landed(uk.at[0:3, 0:128], 11)
    landed(uv.at[0:3, 0:128], 12)
    for d in farthest:
        slot = yp[NY - d]
        wv_t[slot] = uv[slot].T
    for k in range(2):
        @pl.when(z != 2 * y + k)
        def _():
            landed(ctx.at[pl.ds(k * NX, NX)], 4 + k)

    landed(qa.at[0:3], 13)

    def forward_second():
        landed(zkb.at[0, 0:2], 30)
        along_z(-2, 3, right).start()
        along_z(2, 5, left).start()

        @pl.when(z % 2 == 0)
        def _():
            along_z(-2, 4, zp[2]).start()

        @pl.when(z % 2 == 1)
        def _():
            along_z(2, 4, zp[6]).start()

        landed(zkb.at[0, 0:2], 31)
        for o in (1, 7, 2, 6):
            for d in range(1, NX):
                along_x(o, d).start()

    for k in range(NY):
        if k == 2:
            forward_second()
        qt = dot_nt(wq_t[k], qa[...].reshape(QN, 512))
        for h in range(2):
            b = 192 * h
            u = qt[b + 128 : b + 192]
            turned = jnp.concatenate([-u[16:32], u[0:16], -u[48:64], u[32:48]], axis=0)
            rope = u * line_t[:64] + turned * line_t[64:]
            q_t[k, h] = jnp.concatenate(
                [qt[b : b + 128], rope, jnp.zeros((64, QN), F32)], axis=0
            ).astype(BF16)

    def softmax(s_ref, n, k, h, biased):
        parts = [(biased, n, 0.0)]
        if biased:
            parts = [(0, biased, bias_s[pl.ds(k, 1), h : h + 1] * LOG2E)] + parts
        m_old = m_new = m_s[k, h]
        for a, b, lift in parts:
            top = jnp.max(s_ref[a:b], axis=0, keepdims=True) * SCALE2
            m_new = jnp.maximum(m_new, top + lift)
        p = jnp.concatenate(
            [jnp.exp2(s_ref[a:b] * SCALE2 - (m_new - lift)) for a, b, lift in parts], axis=0
        )
        shrink = jnp.exp2(m_old - m_new)
        l_s[k, h] = l_s[k, h] * shrink + jnp.sum(p, axis=0, keepdims=True)
        m_s[k, h] = m_new
        return p.astype(BF16), shrink

    def project(n, k):
        return dot(lows[0:n], uk[k]).astype(BF16), dot_nt(wv_t[k], lows[0:n]).astype(BF16)

    def score(nope, n, k, h):
        key = jnp.concatenate([nope[:, 128 * h : 128 * h + 128], ropes[0:n]], axis=1)
        return dot(key, q_t[k, h])

    def weigh(s_ref, n, k, h, biased):
        p, shrink = softmax(s_ref, n, k, h, biased)
        acc[k, h] = acc[k, h] * shrink + dot(vt[128 * h : 128 * h + 128, 0:n], p)

    def attend(n, stage, biased, passes, finish):
        def step(k, final):
            for at, s, j in passes:
                if final and at == NY - 1:
                    pass_on(s, j)
                elif not final and at < NY - 1:
                    pl.when(k == at)(lambda s=s, j=j: pass_on(s, j))
            sb[0:n] = score(kn[0:n], n, k, 1)
            if not final:
                nope, val = project(n, k + 1)
            weigh(sa, n, k, 0, biased)
            if final:
                finish(k, 0)
            else:
                sa[0:n] = score(nope, n, k + 1, 0)
            weigh(sb, n, k, 1, biased)
            if not final:
                kn[0:n] = nope
                vt[:, 0:n] = val
                finish(k, 0)
            finish(k, 1)

        stage()
        nope, val = project(n, 0)
        kn[0:n] = nope
        vt[:, 0:n] = val
        sa[0:n] = score(nope, n, 0, 0)

        @pl.loop(0, NY - 1)
        def _(k):
            step(k, False)

        step(NY - 1, True)

    def stage_a(at, offset):
        slot = slot_of(offset)
        lows[at : at + BUNDLE] = zka[slot, :, :ROWS_A].reshape(BUNDLE, 256)
        for i in range(NX):
            run = zka[slot, i, ROWS_A:]
            for g in range(4):
                tile = run[:, 128 * (g // 2) : 128 * (g // 2) + 128]
                first = at + ROWS_A * i + 16 * g
                ropes[first : first + 16] = lane_pair(tile) if g % 2 else tile

    def stage_b(at, line):
        lows[at : at + NZ * ROWS_B] = zkb[line, :, :ROWS_B].reshape(NZ * ROWS_B, 256)
        for i in range(NZ):
            tile = zkb[line, i, ROWS_B:, :128]
            first = at + ROWS_B * i
            ropes[first : first + 16] = tile
            ropes[first + 16 : first + 32] = lane_pair(tile)

    def out_copy(k, h, d):
        return remote(ob.at[k, h, yp[d]], rb.at[k, d - 1, h], snd.at[17], rcv.at[34 + k], y=yp[d])

    def stat_copy(k, d):
        return remote(st.at[yp[d], k], rst.at[k, d - 1], snd.at[18], rcv.at[38 + k], y=yp[d])

    def finish(k, h):
        total = l_s[k, h]
        row = m_s[k, h] + jnp.log2(total)
        for j in range(NY):
            st[j, k, h : h + 1] = jnp.concatenate(
                [row[:, ROWS * j : ROWS * j + ROWS], jnp.zeros((1, 32), F32)], axis=1
            )
        ob[k, h] = (acc[k, h] / total).T.astype(BF16).reshape(NY, ROWS, 128)
        for d in farthest:
            if h == 1:
                stat_copy(k, d).start()
            out_copy(k, h, d).start()

    def stage_own():
        both = ctx[...].reshape(CTXK, 384)
        lows[0:CTXK] = both[:, :256]
        ropes[0:CTXK] = both[:, 256:]
        stage_a(CTXK, 0)

    def stage_first():
        stage_b(0, x)
        stage_a(BUNDLE, -1)
        stage_a(2 * BUNDLE, 1)

    def stage_second():
        stage_a(0, -2)
        stage_a(BUNDLE, 2)
        stage_b(2 * BUNDLE, xp[NX - 1])

    def stage_last():
        for i, offset in enumerate((-3, 3, 4)):
            stage_a(i * BUNDLE, offset)
        for d in range(2, NX):
            stage_b((1 + d) * BUNDLE, xp[NX - d])

    def nothing(*_):
        pass

    attend(CTXK + BUNDLE, stage_own, CTXK, ((2, 2, 0), (3, 1, 1)), nothing)
    pass_on(1, 2)
    pass_on(1, 3)
    landed(zkb.at[0, 0:3], 32)
    for d in range(1, NX):
        for o in (3, 5, 4):
            along_x(o, d).start()
    attend(
        3 * BUNDLE, stage_first, 0,
        ((2, 2, 1), (3, 2, 2)), nothing,
    )
    pass_on(2, 3)
    landed(zkb.at[0], 42)
    attend(3 * BUNDLE, stage_second, 0, (), nothing)
    for j in range(NX):
        landed(zka.at[0, 0:2], 25 + j)
    landed(zka.at[0], 29)
    landed(zkb.at[0:2], 33)
    attend(LAST, stage_last, 0, (), finish)

    fetches[16].wait()
    fill = jnp.zeros((6, 128), F32)
    for k in range(NY):
        landed(rst.at[k], 38 + k)
        landed(rb.at[k], 34 + k)
        stats = [st[y, k]] + [rst[k, d - 1] for d in range(1, NY)]
        top = jnp.maximum(jnp.maximum(stats[0], stats[1]), jnp.maximum(stats[2], stats[3]))
        raised = [jnp.exp2(v - top) for v in stats]
        whole = raised[0] + raised[1] + raised[2] + raised[3]
        shares = [jnp.concatenate([r / whole, fill], axis=0).T[:ROWS] for r in raised]
        both = []
        for h in range(2):
            pieces = [ob[k, h, y]] + [rb[k, d - 1, h] for d in range(1, NY)]
            both.append(sum(
                p.astype(F32) * share[:, h : h + 1] for p, share in zip(pieces, shares)
            ))
        part = dot(jnp.concatenate(both, axis=1).astype(BF16), ow[256 * k : 256 * k + 256])
        if k == 0:
            mixed[...] = part
        elif k < NY - 1:
            mixed[...] += part
        else:
            out[...] = (
                lat[...].astype(F32) + gate_s[...] * (mixed[...] + part)
            ).astype(BF16)

    for ref, i in (
        (mod_x.at[0:3], 0), (cx.at[0:3], 1), (mod_z.at[0:7], 2), (mod_y.at[0:3], 3),
        (uq.at[0, 0:192], 5), (uk.at[0:3, 0:128], 6), (uv.at[0:3, 0:128], 7),
        (uq.at[0:3, 0:192], 8), (uq.at[0:3, 0:256], 9), (uk.at[0:3, 0:128], 10),
        (uv.at[0:3, 0:128], 11), (qa.at[0:3], 12), (zka.at[0, 0:3], 13), (zka.at[0:7], 14),
        (zkb.at[0, 0:7], 15), (zkb.at[0:3], 16), (ob.at[:, :, 0:3], 17), (st.at[0:3], 18),
    ):
        drain(ref, i)

    @pl.when(mine)
    def _():
        drain(uq.at[0, 0:448], 4)


def rope_constants():
    inverse = (10000.0 ** (-np.arange(16, dtype=np.float64) / 16)).astype(np.float32)

    def spread(count, first):
        angles = (np.arange(count, dtype=np.float32)[:, None] * inverse).astype(np.float64)
        zero = np.zeros((count, 32))
        runs = []
        for f in (np.cos, np.sin):
            pair = np.concatenate([f(angles), f(angles)], axis=1)
            runs += [pair, zero] if first else [zero, pair]
        return np.concatenate(runs, axis=1).astype(np.float32)

    return spread(192, True), spread(GRID_W, False)


def on_device(
    latent_in, condition, context_latent, context_rope, shift_weight, scale_weight, gate_weight,
    norm_gain, down_query, down_latent, down_rope, query_gain, latent_gain, up_query, up_key,
    up_value, context_bias, out_weight,
):
    row_table, col_table = rope_constants()
    vmem = pltpu.VMEM
    dma = pltpu.SemaphoreType.DMA
    hold = lambda a: pltpu.with_memory_space_constraint(a, pltpu.HBM)
    return pl.pallas_call(
        kernel,
        name="whole",
        out_shape=jax.ShapeDtypeStruct((ROWS, D), BF16),
        in_specs=[pl.BlockSpec(memory_space=pltpu.HBM)] * 20,
        out_specs=pl.BlockSpec(memory_space=pltpu.VMEM),
        scratch_shapes=[
            vmem((1, 64), BF16),
            vmem((64, 512), BF16), vmem((64, 512), BF16), vmem((64, 512), BF16),
            vmem((1, 2), F32),
            vmem((ROWS, D), BF16),
            vmem((1, D), F32), vmem((1, 512), F32), vmem((1, 256), F32),
            vmem((192, 128), F32), vmem((GRID_W, 128), F32),
            vmem((16, 256), BF16), vmem((16, 64), BF16),
            vmem((D, 512), BF16), vmem((D, 256), BF16), vmem((64, D), BF16),
            vmem((1024, D), BF16),
            vmem((NY, 512, 384), BF16), vmem((NY, 256, 256), BF16), vmem((NY, 256, 256), BF16),
            vmem((NX, 3, 512), F32), vmem((NZ, 3, 512), F32), vmem((NY, 4, 512), F32),
            vmem((16, 384), BF16), vmem((NX, 16, 384), BF16), vmem((8, 16, 384), BF16),
            vmem((ROWS, 512), BF16),
            vmem((1, D), F32), vmem((NY, 128), F32),
            vmem((NY, ROWS, 512), BF16),
            vmem((NZ, NX, PIECE_A, 256), BF16), vmem((NX, NZ, PIECE_B, 256), BF16),
            vmem((NY, 384, 512), BF16), vmem((NY, 256, 256), BF16),
            vmem((NY, 2, 256, QN), BF16),
            vmem((LAST, 256), BF16), vmem((LAST, 128), BF16),
            vmem((LAST, 256), BF16), vmem((256, LAST), BF16),
            vmem((LAST, QN), F32), vmem((LAST, QN), F32),
            vmem((NY, 2, 1, QN), F32), vmem((NY, 2, 1, QN), F32),
            vmem((NY, 2, 128, QN), F32),
            vmem((NY, 2, NY, ROWS, 128), BF16), vmem((NY, NY - 1, 2, ROWS, 128), BF16),
            vmem((NY, NY, 2, 128), F32), vmem((NY, NY - 1, 2, 128), F32),
            vmem((ROWS, D), F32),
            dma((17,)), dma((3,)), dma((19,)), dma((43,)),
        ],
        compiler_params=pltpu.CompilerParams(
            collective_id=0, has_side_effects=True, vmem_limit_bytes=40 * 1024 * 1024
        ),
    )(*(hold(a) for a in (
        condition.reshape(1, -1), shift_weight, scale_weight, gate_weight,
        context_bias.reshape(1, -1), latent_in, norm_gain.reshape(1, -1),
        query_gain.reshape(1, -1), latent_gain.reshape(1, -1), jnp.asarray(row_table),
        jnp.asarray(col_table), context_latent, context_rope, down_query, down_latent,
        down_rope.T, up_query, up_key, up_value, out_weight,
    )))


def solution(mesh):
    split = Mesh(mesh.devices.reshape(NZ, NX, NY, 2), ("z", "x", "y", "c"))
    rows = P(("c", "z", "x", "y"), None)
    held = P(("c", "z", "x"), None)
    weight = P(("z", "x"), "y")
    placed = (
        rows, P(("c", "z", "x")), held, held, weight, weight, weight, P(), P(), P(), P(), P(),
        P(), P(None, "y"), P(None, "y"), P(None, "y"), P("y"), P(),
    )
    return jax.shard_map(
        on_device, mesh=split, in_specs=placed, out_specs=rows, check_vma=False
    )
```

```python
import math

import jax
import jax.numpy as jnp
import numpy as np
from jax import lax
from jax.experimental import pallas as pl
from jax.experimental.pallas import tpu as pltpu
from jax.sharding import Mesh
from jax.sharding import PartitionSpec as P

ROWS = 96
D = 2048
NZ, NX, NY = 8, 4, 4
GRID_W = 64
CTXK = 128
EPS = 1e-06
QN = NY * ROWS
ROWS_A, ROWS_B = 64, 32
PIECE_A, PIECE_B = ROWS_A + 16, ROWS_B + 16
BUNDLE = NX * ROWS_A
LAST = 3 * BUNDLE + (NX - 2) * NZ * ROWS_B
LOG2E = math.log2(math.e)
SCALE2 = LOG2E / math.sqrt(192.0)
MESH = pl.DeviceIdType.MESH
F32 = jnp.float32
BF16 = jnp.bfloat16
NEG = float("-inf")


def dot(a, b):
    return jnp.dot(a, b, preferred_element_type=F32)


def dot_nt(a, b):
    return lax.dot_general(a, b, (((1,), (1,)), ((), ())), preferred_element_type=F32)


def remote(src, dst, send_sem, recv_sem, **where):
    return pltpu.make_async_remote_copy(
        src_ref=src, dst_ref=dst, send_sem=send_sem, recv_sem=recv_sem,
        device_id=where, device_id_type=MESH,
    )


def lane_pair(run):
    return jnp.concatenate([run[:, 64:], run[:, :64]], axis=1)


def piece_order(k):
    return k + (k // 2) * (5 - 2 * k)


def kernel(
    cond_h, sw_h, cw_h, gw_h, bias_h, lat_h, gain_h, qg_h, lg_h, rowt_h, colt_h, ctxl_h, ctxr_h,
    dq_h, dl_h, dr_h, uq_h, uk_h, uv_h, ow_h,
    out,
    cond, sw, cw, gw, bias, lat, gain, qg, lg, rowt, colt, ctxl, ctxr, dq, dl, dr, ow,
    uq, uk, uv, mod_x, mod_z, mod_y, cblk, cx, ctx, qlow, gate_s, bias_s,
    qa, zka, zkb, wq_t, wv_t, q_t, lows, ropes, kn, vt, sa, sb, m_s, l_s, acc, ob, rb, st, rst, mixed,
    in_sem, own_sem, snd, rcv,
):
    z, x, y, c = (lax.axis_index(n) for n in ("z", "x", "y", "c"))
    sp = z * NX + x

    def drain(ref, i):
        remote(ref, ref, snd.at[i], rcv.at[0], c=1 - c).wait_send()

    def landed(ref, i):
        remote(ref, ref, snd.at[0], rcv.at[i], c=1 - c).wait_recv()

    fetches = [
        pltpu.make_async_copy(h, v, in_sem.at[i])
        for i, (h, v) in enumerate((
            (cond_h, cond), (sw_h, sw), (cw_h, cw), (gw_h, gw), (bias_h, bias), (ctxl_h, ctxl),
            (ctxr_h, ctxr), (lat_h, lat), (gain_h, gain), (qg_h, qg), (lg_h, lg),
            (rowt_h, rowt), (colt_h, colt), (dq_h, dq), (dl_h, dl), (dr_h, dr), (ow_h, ow),
        ))
    ]
    owns = [
        pltpu.make_async_copy(h, v.at[y], own_sem.at[i])
        for i, (h, v) in enumerate(((uq_h, uq), (uk_h, uk), (uv_h, uv)))
    ]
    for copy in fetches[:7] + owns:
        copy.start()
    xp = [lax.rem(x + d, NX) for d in range(NX)]
    yp = [lax.rem(y + d, NY) for d in range(NY)]
    zp = [lax.rem(z + d, NZ) for d in range(NZ)]
    right, left = zp[1], zp[NZ - 1]
    farthest = (2, 1, 3)
    peers = (
        [{"x": xp[d]} for d in range(1, NX)]
        + [{"y": yp[d]} for d in range(1, NY)]
        + [{"z": zp[d]} for d in range(1, NZ)]
        + [{"c": 1 - c}]
    )
    barrier = pltpu.get_barrier_semaphore()
    for where in peers:
        pl.semaphore_signal(barrier, inc=1, device_id=where, device_id_type=MESH)

    for copy in fetches[:7]:
        copy.wait()
    v = cond[...].astype(F32)
    activated = (v / (1.0 + jnp.exp(-v))).astype(BF16)
    mod_x[x] = jnp.concatenate([dot(activated, w[...]) for w in (sw, cw, gw)], axis=0)
    pl.semaphore_wait(barrier, len(peers))
    xcopies = [
        remote(mod_x.at[x], mod_x.at[x], snd.at[0], rcv.at[0], x=xp[d]) for d in farthest
    ]
    for copy in xcopies:
        copy.start()
    for copy in fetches[7:]:
        copy.start()
    for copy in owns:
        copy.wait()
    cblk[...] = jnp.concatenate([ctxl[...], ctxr[...], jnp.zeros((16, 64), BF16)], axis=1)
    cx[x] = cblk[...]
    ccopies = [remote(cblk, cx.at[x], snd.at[1], rcv.at[1], x=xp[d]) for d in farthest]
    for copy in ccopies:
        copy.start()

    def half(ref, slot):
        rows = ref.shape[1] // 2
        return ref.at[slot, pl.ds(pl.multiple_of(c * rows, rows), rows)]

    def eighth(slot):
        return uq.at[slot, pl.ds(pl.multiple_of(c * 256 + x * 64, 64), 64)]

    def over_y(d, i):
        return remote(half(ups[i], y), half(ups[i], y), snd.at[5 + i], rcv.at[6 + i], y=yp[d])

    def eighth_over_y(d):
        return remote(eighth(y), eighth(y), snd.at[5], rcv.at[6], y=yp[d])

    def eighth_over_x(d, e):
        slot = yp[NY - d]
        return remote(eighth(slot), eighth(slot), snd.at[8], rcv.at[9], x=xp[e])

    def across(d, i):
        slot = yp[NY - d]
        return remote(half(ups[i], slot), half(ups[i], slot), snd.at[9 + i], rcv.at[10 + i], c=1 - c)

    ups = (uq, uk, uv)
    for d in farthest:
        eighth_over_y(d).start()
    for d in farthest:
        over_y(d, 1).start()

    landed(mod_x.at[0:3], 0)
    mod_z[z] = mod_x[0] + mod_x[1] + mod_x[2] + mod_x[3]
    zcopies = [
        remote(mod_z.at[z], mod_z.at[z], snd.at[2], rcv.at[2], z=zp[d])
        for d in (4, 3, 5, 2, 6, 1, 7)
    ]
    for copy in zcopies:
        copy.start()
    for copy in fetches[7:13]:
        copy.wait()
    lat32 = lat[...].astype(F32)
    inv = lax.rsqrt(jnp.mean(lat32 * lat32, axis=-1, keepdims=True) + EPS)
    scaled = lat32 * inv * gain[...]
    line = [rowt[pl.ds(sp * 6 + i, 1), :] + colt[...] for i in range(6)]
    line_t = jnp.concatenate(line, axis=0).T
    own_table = []
    for t in range(3):
        g = y * 3 + t
        own_table.append(
            rowt[pl.ds(sp * 6 + g // 2, 1), :]
            + colt[pl.ds(pl.multiple_of((g % 2) * 32, 32), 32), :]
        )
    own_table = jnp.concatenate(own_table, axis=0)
    wq_t[y] = uq[y].T
    wv_t[y] = uv[y].T
    m_s[...] = jnp.full(m_s.shape, NEG, F32)
    l_s[...] = jnp.zeros(l_s.shape, F32)
    acc[...] = jnp.zeros(acc.shape, F32)
    landed(cx.at[0:3], 1)
    mine = z // 2 == y
    zc = [
        remote(
            cx, ctx.at[pl.ds(pl.multiple_of((z % 2) * NX, NX), NX)], snd.at[4],
            rcv.at[4 + z % 2], z=zp[d],
        )
        for d in range(1, NZ)
    ]

    @pl.when(mine)
    def _():
        ctx[pl.ds((z % 2) * NX, NX)] = cx[...]
        for copy in zc:
            copy.start()

    landed(uq.at[0, 0:192], 6)
    for d in farthest:
        for e in farthest:
            eighth_over_x(d, e).start()

    landed(mod_z.at[0:7], 2)
    total = mod_z[0]
    for k in range(1, NZ):
        total = total + mod_z[k]
    bias_row = jnp.concatenate([bias[...], jnp.zeros((1, 510), F32)], axis=1)
    mod_y[y] = jnp.concatenate([total, bias_row], axis=0)
    ycopies = [
        remote(mod_y.at[y], mod_y.at[y], snd.at[3], rcv.at[3], y=yp[d]) for d in farthest
    ]
    for copy in ycopies:
        copy.start()
    for d in farthest:
        over_y(d, 2).start()
    landed(uk.at[0:3, 0:128], 7)
    for d in farthest:
        across(d, 1).start()

    landed(mod_y.at[0:3], 3)
    landed(uq.at[0:3, 0:192], 9)
    for d in farthest:
        across(d, 0).start()
    shift = jnp.concatenate([mod_y[k, 0:1] for k in range(NY)], axis=1)
    scale = jnp.concatenate([mod_y[k, 1:2] for k in range(NY)], axis=1)
    gate_s[...] = jnp.concatenate([mod_y[k, 2:3] for k in range(NY)], axis=1)
    bias_s[...] = jnp.concatenate([mod_y[k, 3:4, 0:128] for k in range(NY)], axis=0)
    normed = (scaled * (1.0 + scale) + shift).astype(BF16)
    for copy in fetches[13:16]:
        copy.wait()

    def rms(a, g):
        return a * lax.rsqrt(jnp.mean(a * a, axis=-1, keepdims=True) + EPS) * g

    qlow[...] = rms(dot(normed, dq[...]), qg[...]).astype(BF16)
    qcopies = [remote(qlow, qa.at[y], snd.at[12], rcv.at[13], y=yp[d]) for d in farthest]
    for copy in qcopies:
        copy.start()
    low = rms(dot(normed, dl[...]), lg[...]).astype(BF16)
    u = dot_nt(normed, dr[...])
    turned = jnp.concatenate([-u[:, 16:32], u[:, 0:16], -u[:, 48:64], u[:, 32:48]], axis=1)
    rope = u * own_table[:, :64] + turned * own_table[:, 64:]
    runs = [rope[16 * g : 16 * g + 16] for g in range(6)]
    zka[z, x] = jnp.concatenate(
        [low[:ROWS_A], jnp.concatenate(runs[:4], axis=1).astype(BF16)], axis=0
    )
    zkb[x, z] = jnp.concatenate(
        [
            low[ROWS_A:],
            jnp.concatenate(runs[4:] + [jnp.zeros((16, 128), F32)], axis=1).astype(BF16),
        ],
        axis=0,
    )

    def slot_of(offset):
        return lax.rem(z + offset + NZ, NZ)

    def piece(offset, j):
        return zka.at[slot_of(offset), lax.rem(x - piece_order(j) + NX, NX)]

    def turn(s, j):
        return rcv.at[13 + 4 * s + j]

    def go_right(s, j):
        return remote(piece(1 - s, j), piece(1 - s, j), snd.at[14], turn(s, j), z=right)

    def go_left(s, j):
        return remote(piece(s - 1, j), piece(s - 1, j), snd.at[14], turn(s, j), z=left)

    def two_right(j):
        return remote(piece(-2, j), piece(-2, j), snd.at[14], rcv.at[29], z=zp[2])

    def two_left(j):
        return remote(piece(2, j), piece(2, j), snd.at[14], rcv.at[29], z=zp[NZ - 2])

    def pass_on(s, j):
        landed(zka.at[0, 0:2], 13 + 4 * s + j)
        go_right(s + 1, j).start()
        go_left(s + 1, j).start()
        if s == 2:
            (two_right if j < 2 else two_left)(j).start()

    kcopies = [
        remote(zka.at[z, x], zka.at[z, x], snd.at[13], rcv.at[13 + d], x=xp[d]) for d in range(1, NX)
    ]
    def along_z(origin, d, to):
        held = zkb.at[x, slot_of(origin)]
        group = 30 if d in (2, 6) else 31 if d in (1, 7) else 32
        return remote(held, held, snd.at[15], rcv.at[group], z=to)

    def along_x(o, d):
        held = zkb.at[x, slot_of(-o)]
        return remote(held, held, snd.at[16], rcv.at[42 if d == 1 else 33], x=xp[d])

    for d in farthest:
        kcopies[d - 1].start()
    go_right(1, 0).start()
    go_left(1, 0).start()
    for d in (2, 6, 1, 7):
        along_z(0, d, zp[d]).start()
    for d in farthest:
        along_x(0, d).start()
    qa[y] = qlow[...]

    landed(uv.at[0:3, 0:128], 8)
    for d in farthest:
        across(d, 2).start()
    landed(uq.at[0:3, 0:256], 10)
    for d in farthest:
        slot = yp[NY - d]
        wq_t[slot] = uq[slot].T
    pass_on(1, 0)
    for j, d in ((1, 1), (2, 3), (3, 2)):
        kcopies[d - 1].wait_recv()
        go_right(1, j).start()
        go_left(1, j).start()
    landed(uk.at[0:3, 0:128], 11)
    landed(uv.at[0:3, 0:128], 12)
    for d in farthest:
        slot = yp[NY - d]
        wv_t[slot] = uv[slot].T
    for k in range(2):
        @pl.when(z != 2 * y + k)
        def _():
            landed(ctx.at[pl.ds(k * NX, NX)], 4 + k)

    landed(qa.at[0:3], 13)

    def forward_second():
        landed(zkb.at[0, 0:2], 30)

        @pl.when(z % 2 == 0)
        def _():
            along_z(-2, 4, zp[2]).start()

        @pl.when(z % 2 == 1)
        def _():
            along_z(2, 4, zp[6]).start()

        along_z(-2, 3, right).start()
        along_z(2, 5, left).start()

        landed(zkb.at[0, 0:2], 31)
        for o in (1, 7, 2, 6):
            for d in range(1, NX):
                along_x(o, d).start()

    for k in range(NY):
        if k == 1:
            forward_second()
        qt = dot_nt(wq_t[k], qa[...].reshape(QN, 512))
        for h in range(2):
            b = 192 * h
            u = qt[b + 128 : b + 192]
            turned = jnp.concatenate([-u[16:32], u[0:16], -u[48:64], u[32:48]], axis=0)
            rope = u * line_t[:64] + turned * line_t[64:]
            q_t[k, h] = jnp.concatenate(
                [qt[b : b + 128], rope, jnp.zeros((64, QN), F32)], axis=0
            ).astype(BF16)

    def softmax(s_ref, n, k, h, biased):
        parts = [(biased, n, 0.0)]
        if biased:
            parts = [(0, biased, bias_s[pl.ds(k, 1), h : h + 1] * LOG2E)] + parts
        m_old = m_new = m_s[k, h]
        for a, b, lift in parts:
            top = jnp.max(s_ref[a:b], axis=0, keepdims=True) * SCALE2
            m_new = jnp.maximum(m_new, top + lift)
        p = jnp.concatenate(
            [jnp.exp2(s_ref[a:b] * SCALE2 - (m_new - lift)) for a, b, lift in parts], axis=0
        )
        shrink = jnp.exp2(m_old - m_new)
        l_s[k, h] = l_s[k, h] * shrink + jnp.sum(p, axis=0, keepdims=True)
        m_s[k, h] = m_new
        return p.astype(BF16), shrink

    def project(n, k):
        return dot(lows[0:n], uk[k]).astype(BF16), dot_nt(wv_t[k], lows[0:n]).astype(BF16)

    def score(nope, n, k, h):
        key = jnp.concatenate([nope[:, 128 * h : 128 * h + 128], ropes[0:n]], axis=1)
        return dot(key, q_t[k, h])

    def weigh(s_ref, n, k, h, biased):
        p, shrink = softmax(s_ref, n, k, h, biased)
        acc[k, h] = acc[k, h] * shrink + dot(vt[128 * h : 128 * h + 128, 0:n], p)

    def attend(n, stage, biased, passes, finish):
        def step(k, final):
            for at, s, j in passes:
                if final and at == NY - 1:
                    pass_on(s, j)
                elif not final and at < NY - 1:
                    pl.when(k == at)(lambda s=s, j=j: pass_on(s, j))
            sb[0:n] = score(kn[0:n], n, k, 1)
            if not final:
                nope, val = project(n, k + 1)
            weigh(sa, n, k, 0, biased)
            if final:
                finish(k, 0)
            else:
                sa[0:n] = score(nope, n, k + 1, 0)
            weigh(sb, n, k, 1, biased)
            if not final:
                kn[0:n] = nope
                vt[:, 0:n] = val
                finish(k, 0)
            finish(k, 1)

        stage()
        nope, val = project(n, 0)
        kn[0:n] = nope
        vt[:, 0:n] = val
        sa[0:n] = score(nope, n, 0, 0)

        @pl.loop(0, NY - 1)
        def _(k):
            step(k, False)

        step(NY - 1, True)

    def stage_a(at, offset):
        slot = slot_of(offset)
        lows[at : at + BUNDLE] = zka[slot, :, :ROWS_A].reshape(BUNDLE, 256)
        for i in range(NX):
            run = zka[slot, i, ROWS_A:]
            for g in range(4):
                tile = run[:, 128 * (g // 2) : 128 * (g // 2) + 128]
                first = at + ROWS_A * i + 16 * g
                ropes[first : first + 16] = lane_pair(tile) if g % 2 else tile

    def stage_b(at, line):
        lows[at : at + NZ * ROWS_B] = zkb[line, :, :ROWS_B].reshape(NZ * ROWS_B, 256)
        for i in range(NZ):
            tile = zkb[line, i, ROWS_B:, :128]
            first = at + ROWS_B * i
            ropes[first : first + 16] = tile
            ropes[first + 16 : first + 32] = lane_pair(tile)

    def out_copy(k, h, d):
        return remote(ob.at[k, h, yp[d]], rb.at[k, d - 1, h], snd.at[17], rcv.at[34 + k], y=yp[d])

    def stat_copy(k, d):
        return remote(st.at[yp[d], k], rst.at[k, d - 1], snd.at[18], rcv.at[38 + k], y=yp[d])

    def finish(k, h):
        total = l_s[k, h]
        row = m_s[k, h] + jnp.log2(total)
        for j in range(NY):
            st[j, k, h : h + 1] = jnp.concatenate(
                [row[:, ROWS * j : ROWS * j + ROWS], jnp.zeros((1, 32), F32)], axis=1
            )
        ob[k, h] = (acc[k, h] / total).T.astype(BF16).reshape(NY, ROWS, 128)
        for d in farthest:
            if h == 1:
                stat_copy(k, d).start()
            out_copy(k, h, d).start()

    def stage_own():
        both = ctx[...].reshape(CTXK, 384)
        lows[0:CTXK] = both[:, :256]
        ropes[0:CTXK] = both[:, 256:]
        stage_a(CTXK, 0)

    def stage_first():
        stage_b(0, x)
        stage_a(BUNDLE, -1)
        stage_a(2 * BUNDLE, 1)

    def stage_second():
        stage_a(0, -2)
        stage_a(BUNDLE, 2)
        stage_b(2 * BUNDLE, xp[NX - 1])

    def stage_last():
        for i, offset in enumerate((-3, 3, 4)):
            stage_a(i * BUNDLE, offset)
        for d in range(2, NX):
            stage_b((1 + d) * BUNDLE, xp[NX - d])

    def nothing(*_):
        pass

    attend(CTXK + BUNDLE, stage_own, CTXK, ((2, 2, 0), (3, 1, 1)), nothing)
    pass_on(1, 2)
    pass_on(1, 3)
    landed(zkb.at[0, 0:3], 32)
    for d in range(1, NX):
        for o in (3, 5, 4):
            along_x(o, d).start()
    attend(
        3 * BUNDLE, stage_first, 0,
        ((2, 2, 1), (3, 2, 2)), nothing,
    )
    pass_on(2, 3)
    landed(zkb.at[0], 42)
    attend(3 * BUNDLE, stage_second, 0, (), nothing)
    for j in range(NX):
        landed(zka.at[0, 0:2], 25 + j)
    landed(zka.at[0], 29)
    landed(zkb.at[0:2], 33)
    attend(LAST, stage_last, 0, (), finish)

    fetches[16].wait()
    fill = jnp.zeros((6, 128), F32)
    for k in range(NY):
        landed(rst.at[k], 38 + k)
        landed(rb.at[k], 34 + k)
        stats = [st[y, k]] + [rst[k, d - 1] for d in range(1, NY)]
        top = jnp.maximum(jnp.maximum(stats[0], stats[1]), jnp.maximum(stats[2], stats[3]))
        raised = [jnp.exp2(v - top) for v in stats]
        whole = raised[0] + raised[1] + raised[2] + raised[3]
        shares = [jnp.concatenate([r / whole, fill], axis=0).T[:ROWS] for r in raised]
        both = []
        for h in range(2):
            pieces = [ob[k, h, y]] + [rb[k, d - 1, h] for d in range(1, NY)]
            both.append(sum(
                p.astype(F32) * share[:, h : h + 1] for p, share in zip(pieces, shares)
            ))
        part = dot(jnp.concatenate(both, axis=1).astype(BF16), ow[256 * k : 256 * k + 256])
        if k == 0:
            mixed[...] = part
        elif k < NY - 1:
            mixed[...] += part
        else:
            out[...] = (
                lat[...].astype(F32) + gate_s[...] * (mixed[...] + part)
            ).astype(BF16)

    for ref, i in (
        (mod_x.at[0:3], 0), (cx.at[0:3], 1), (mod_z.at[0:7], 2), (mod_y.at[0:3], 3),
        (uq.at[0, 0:192], 5), (uk.at[0:3, 0:128], 6), (uv.at[0:3, 0:128], 7),
        (uq.at[0:3, 0:192], 8), (uq.at[0:3, 0:256], 9), (uk.at[0:3, 0:128], 10),
        (uv.at[0:3, 0:128], 11), (qa.at[0:3], 12), (zka.at[0, 0:3], 13), (zka.at[0:7], 14),
        (zkb.at[0, 0:7], 15), (zkb.at[0:3], 16), (ob.at[:, :, 0:3], 17), (st.at[0:3], 18),
    ):
        drain(ref, i)

    @pl.when(mine)
    def _():
        drain(uq.at[0, 0:448], 4)


def rope_constants():
    inverse = (10000.0 ** (-np.arange(16, dtype=np.float64) / 16)).astype(np.float32)

    def spread(count, first):
        angles = (np.arange(count, dtype=np.float32)[:, None] * inverse).astype(np.float64)
        zero = np.zeros((count, 32))
        runs = []
        for f in (np.cos, np.sin):
            pair = np.concatenate([f(angles), f(angles)], axis=1)
            runs += [pair, zero] if first else [zero, pair]
        return np.concatenate(runs, axis=1).astype(np.float32)

    return spread(192, True), spread(GRID_W, False)


def on_device(
    latent_in, condition, context_latent, context_rope, shift_weight, scale_weight, gate_weight,
    norm_gain, down_query, down_latent, down_rope, query_gain, latent_gain, up_query, up_key,
    up_value, context_bias, out_weight,
):
    row_table, col_table = rope_constants()
    vmem = pltpu.VMEM
    dma = pltpu.SemaphoreType.DMA
    hold = lambda a: pltpu.with_memory_space_constraint(a, pltpu.HBM)
    return pl.pallas_call(
        kernel,
        name="whole",
        out_shape=jax.ShapeDtypeStruct((ROWS, D), BF16),
        in_specs=[pl.BlockSpec(memory_space=pltpu.HBM)] * 20,
        out_specs=pl.BlockSpec(memory_space=pltpu.VMEM),
        scratch_shapes=[
            vmem((1, 64), BF16),
            vmem((64, 512), BF16), vmem((64, 512), BF16), vmem((64, 512), BF16),
            vmem((1, 2), F32),
            vmem((ROWS, D), BF16),
            vmem((1, D), F32), vmem((1, 512), F32), vmem((1, 256), F32),
            vmem((192, 128), F32), vmem((GRID_W, 128), F32),
            vmem((16, 256), BF16), vmem((16, 64), BF16),
            vmem((D, 512), BF16), vmem((D, 256), BF16), vmem((64, D), BF16),
            vmem((1024, D), BF16),
            vmem((NY, 512, 384), BF16), vmem((NY, 256, 256), BF16), vmem((NY, 256, 256), BF16),
            vmem((NX, 3, 512), F32), vmem((NZ, 3, 512), F32), vmem((NY, 4, 512), F32),
            vmem((16, 384), BF16), vmem((NX, 16, 384), BF16), vmem((8, 16, 384), BF16),
            vmem((ROWS, 512), BF16),
            vmem((1, D), F32), vmem((NY, 128), F32),
            vmem((NY, ROWS, 512), BF16),
            vmem((NZ, NX, PIECE_A, 256), BF16), vmem((NX, NZ, PIECE_B, 256), BF16),
            vmem((NY, 384, 512), BF16), vmem((NY, 256, 256), BF16),
            vmem((NY, 2, 256, QN), BF16),
            vmem((LAST, 256), BF16), vmem((LAST, 128), BF16),
            vmem((LAST, 256), BF16), vmem((256, LAST), BF16),
            vmem((LAST, QN), F32), vmem((LAST, QN), F32),
            vmem((NY, 2, 1, QN), F32), vmem((NY, 2, 1, QN), F32),
            vmem((NY, 2, 128, QN), F32),
            vmem((NY, 2, NY, ROWS, 128), BF16), vmem((NY, NY - 1, 2, ROWS, 128), BF16),
            vmem((NY, NY, 2, 128), F32), vmem((NY, NY - 1, 2, 128), F32),
            vmem((ROWS, D), F32),
            dma((17,)), dma((3,)), dma((19,)), dma((43,)),
        ],
        compiler_params=pltpu.CompilerParams(
            collective_id=0, has_side_effects=True, vmem_limit_bytes=40 * 1024 * 1024
        ),
    )(*(hold(a) for a in (
        condition.reshape(1, -1), shift_weight, scale_weight, gate_weight,
        context_bias.reshape(1, -1), latent_in, norm_gain.reshape(1, -1),
        query_gain.reshape(1, -1), latent_gain.reshape(1, -1), jnp.asarray(row_table),
        jnp.asarray(col_table), context_latent, context_rope, down_query, down_latent,
        down_rope.T, up_query, up_key, up_value, out_weight,
    )))


def solution(mesh):
    split = Mesh(mesh.devices.reshape(NZ, NX, NY, 2), ("z", "x", "y", "c"))
    rows = P(("c", "z", "x", "y"), None)
    held = P(("c", "z", "x"), None)
    weight = P(("z", "x"), "y")
    placed = (
        rows, P(("c", "z", "x")), held, held, weight, weight, weight, P(), P(), P(), P(), P(),
        P(), P(None, "y"), P(None, "y"), P(None, "y"), P("y"), P(),
    )
    return jax.shard_map(
        on_device, mesh=split, in_specs=placed, out_specs=rows, check_vma=False
    )
```
